32 devices in a mesh: rep: 2 (over x), fs: 4 (over z), tp: 4 (over y, core).
Axes of the slice: x: 2, y: 2, z: 4, core: 2. Of those that a mesh axis runs over, the one named last changes fastest.
Arguments:
- stream: bfloat16 [4096, 2048], P(('rep', 'fs', 'tp')), may hold values from -6 to 6
- gate_weight: bfloat16 [2048, 2816], P('fs', 'tp'), may hold values from -0.125 to 0.125
- up_weight: bfloat16 [2048, 2816], P('fs', 'tp'), may hold values from -0.125 to 0.125
- down_weight: bfloat16 [2816, 2048], P('tp', 'fs'), may hold values from -0.21875 to 0.21875
- query_weight: bfloat16 [2048, 512], P('fs', 'tp'), may hold values from -0.125 to 0.125
- key_weight: bfloat16 [2048, 512], P('fs', 'tp'), may hold values from -0.125 to 0.125
- value_weight: bfloat16 [2048, 1024], P('fs', 'tp'), may hold values from -0.125 to 0.125
- outgate_weight: bfloat16 [2048, 1024], P('fs', 'tp'), may hold values from -0.125 to 0.125
- decay_down: bfloat16 [2048, 32], replicated, may hold values from -0.125 to 0.125
- decay_up: bfloat16 [32, 512], P(None, 'tp'), may hold values from -2 to 2
- decay_bias: float32 [512], P('tp'), may hold values from -0.5 to 7
- head_gain: float32 [128], replicated, may hold values from 0.1 to 1.9
- out_weight: bfloat16 [1024, 2048], P('tp', 'fs'), may hold values from -0.375 to 0.375
- norm_gain: float32 [3, 2048], replicated, may hold values from 0.1 to 1.9
Outputs:
- layer_out: bfloat16 [4096, 2048], P(('rep', 'fs', 'tp'))
The draws below stay inside these ranges and needn't reach their ends.
All inputs are finite; a program needn't handle non-finite values.
Results may differ from the reference program's by a relative error of at most 0.015.
Values may be sent and summed in bfloat16 or wider, within the bound.
A program may use at most 128 MiB of HBM per device.

```python
import jax
import jax.numpy as jnp
from jax import lax

D = 2048
FF = 2816
HEADS = 8
DK = 64
DV = 128
GR = 32
BLOCK = 64
KW = 512
VW = 1024
SEQLEN = 512
SEQS = 8
TOKENS = 4096


def draw_decay_bias(key, part):
    pick_key, fast_key, slow_key = jax.random.split(key, 3)
    share = 0.5
    quick = jax.random.uniform(pick_key, (HEADS, 1), jnp.float32) < share
    fast_values = jax.random.uniform(fast_key, (HEADS, DK), jnp.float32, -0.5, 1.5)
    slow_values = jax.random.uniform(slow_key, (HEADS, DK), jnp.float32, 4.0, 7.0)
    return jnp.where(quick, fast_values, slow_values).reshape(HEADS * DK)


def shard_levels(rng, extent, cuts, least, top_value):
    gain, own = 1.0, jax.random.fold_in(rng, 6)
    for axis_at, parts in cuts:
        steps = jnp.exp(jax.random.uniform(jax.random.fold_in(own, axis_at), (parts,), jnp.float32, least / len(cuts), top_value / len(cuts)))
        gain = gain * jnp.repeat(steps, extent[axis_at] // parts).reshape([-1 if axis == axis_at else 1 for axis in range(len(extent))])
    return gain


def scatter_about(own_key, dims, width, reach, cuts=(), kind=jnp.bfloat16):
    entries = width * jax.random.normal(own_key, dims, jnp.float32)
    if cuts:
        entries = entries * shard_levels(own_key, dims, cuts, -0.22, 0.18)
    return jnp.clip(entries, -reach, reach).astype(kind)


def setup_inputs(seed: int = 0) -> dict:
    arg_keys = jax.random.split(jax.random.key(seed), 15)
    return {
        "stream": scatter_about(arg_keys[0], (TOKENS, D), 1.0, 6.0, ((0, 32),)),
        "gate_weight": scatter_about(arg_keys[1], (D, FF), D ** -0.5, 0.125, ((0, 4), (1, 4))),
        "up_weight": scatter_about(arg_keys[2], (D, FF), D ** -0.5, 0.125, ((0, 4), (1, 4))),
        "down_weight": scatter_about(arg_keys[3], (FF, D), (FF // 4) ** -0.5, 0.21875, ((0, 4), (1, 4))),
        "query_weight": scatter_about(arg_keys[4], (D, KW), D ** -0.5, 0.125, ((0, 4), (1, 4))),
        "key_weight": scatter_about(arg_keys[5], (D, KW), D ** -0.5, 0.125, ((0, 4), (1, 4))),
        "value_weight": scatter_about(arg_keys[6], (D, VW), D ** -0.5, 0.125, ((0, 4), (1, 4))),
        "outgate_weight": scatter_about(arg_keys[7], (D, VW), D ** -0.5, 0.125, ((0, 4), (1, 4))),
        "decay_down": scatter_about(arg_keys[8], (D, GR), D ** -0.5, 0.125),
        "decay_up": scatter_about(arg_keys[9], (GR, KW), (GR // 4) ** -0.5, 2.0, ((1, 4),)),
        "decay_bias": draw_decay_bias(jax.random.fold_in(arg_keys[14], 71), 0),
        "head_gain": jnp.clip(1.0 + 0.18 * jax.random.normal(arg_keys[11], (DV,), jnp.float32), 0.1, 1.9),
        "out_weight": scatter_about(arg_keys[12], (VW, D), (VW // 4) ** -0.5, 0.375, ((0, 4), (1, 4))),
        "norm_gain": jnp.clip(1.0 + 0.18 * jax.random.normal(arg_keys[13], (3, D), jnp.float32), 0.1, 1.9),
    }


RESIDUAL_SCALE = 2.0 ** 0.5
BRANCH_SCALE = 0.5
NORM_EPS = 1e-05
HEAD_EPS = 0.01
GATE_DIVISOR = 16.0

def layer_norm(values, norm_scale):
    average = lax.optimization_barrier(jnp.mean(values, -1, keepdims=True))
    centred = values - average
    spread = lax.optimization_barrier(jnp.mean(centred * centred, -1, keepdims=True))
    return (centred * lax.rsqrt(spread + NORM_EPS) * norm_scale).astype(jnp.bfloat16)

def blocked_mixer(query, key_rows, value_rows, log_gate):
    length, head_count, key_dim = query.shape
    value_dim = value_rows.shape[2]
    block_count = length // BLOCK
    highest = lax.Precision.HIGHEST

    def split_blocks(values):
        return values.reshape(block_count, BLOCK, head_count, values.shape[2]).transpose(0, 2, 1, 3)
    causal = jnp.tril(jnp.ones((BLOCK, BLOCK), dtype=bool))

    def advance(carried, inputs):
        query_blk, key_blk, value_blk, decay_blk = inputs
        log_gaps = decay_blk[:, :, None, :] - decay_blk[:, None, :, :]
        log_gaps = jnp.where(causal[None, :, :, None], log_gaps, -jnp.inf)
        scores = lax.optimization_barrier(jnp.sum(query_blk[:, :, None, :] * key_blk[:, None, :, :] * jnp.exp(log_gaps), axis=-1))
        inside = jnp.einsum('hij,hjv->hiv', scores, value_blk, precision=highest)
        carried_part = jnp.einsum('hid,hdv->hiv', query_blk * jnp.exp(decay_blk), carried, precision=highest)
        closing = decay_blk[:, -1, :]
        update = jnp.einsum('hjd,hjv->hdv', key_blk * jnp.exp(closing[:, None, :] - decay_blk), value_blk, precision=highest)
        return (carried * jnp.exp(closing)[:, :, None] + update, inside + carried_part)
    cumulative = jnp.cumsum(split_blocks(log_gate), axis=2)
    start_state = jnp.zeros((head_count, key_dim, value_dim), jnp.float32)
    _, outputs = lax.scan(advance, start_state, (split_blocks(query), split_blocks(key_rows), split_blocks(value_rows), cumulative))
    return outputs.transpose(0, 2, 1, 3).reshape(length, head_count, value_dim)

def reference(stream, gate_weight, up_weight, down_weight, query_weight, key_weight, value_weight, outgate_weight, decay_down, decay_up, decay_bias, head_gain, out_weight, norm_gain):

    def ffn_half(current, norm_scale):
        gate = jnp.dot(current, gate_weight, preferred_element_type=jnp.float32)
        upward = jnp.dot(current, up_weight, preferred_element_type=jnp.float32)
        hidden = (jax.nn.silu(gate) * upward).astype(jnp.bfloat16)
        summed = jnp.dot(hidden, down_weight, preferred_element_type=jnp.float32)
        return layer_norm(RESIDUAL_SCALE * current.astype(jnp.float32) + BRANCH_SCALE * summed, norm_scale)

    def one_sequence(sequence):
        first = ffn_half(sequence, norm_gain[0])
        query = jnp.dot(first, query_weight, preferred_element_type=jnp.float32).astype(jnp.bfloat16)
        key_rows = jnp.dot(first, key_weight, preferred_element_type=jnp.float32).astype(jnp.bfloat16)
        value_rows = jnp.dot(first, value_weight, preferred_element_type=jnp.float32).astype(jnp.bfloat16)
        outgate = jnp.dot(first, outgate_weight, preferred_element_type=jnp.float32).astype(jnp.bfloat16)
        low_rank = jnp.dot(first, decay_down, preferred_element_type=jnp.float32).astype(jnp.bfloat16)
        pre_gate = jnp.dot(low_rank, decay_up, preferred_element_type=jnp.float32) + decay_bias
        log_gate = jax.nn.log_sigmoid(pre_gate) / GATE_DIVISOR
        length = first.shape[0]
        mixed = blocked_mixer(query.astype(jnp.float32).reshape(length, HEADS, DK) * DK ** (-0.5), key_rows.astype(jnp.float32).reshape(length, HEADS, DK), value_rows.astype(jnp.float32).reshape(length, HEADS, DV), log_gate.reshape(length, HEADS, DK))
        normed = mixed * lax.rsqrt(lax.optimization_barrier(jnp.mean(mixed * mixed, -1, keepdims=True)) + HEAD_EPS) * head_gain
        gated = (normed.reshape(length, HEADS * DV) * jax.nn.silu(outgate.astype(jnp.float32))).astype(jnp.bfloat16)
        summed = jnp.dot(gated, out_weight, preferred_element_type=jnp.float32)
        second = layer_norm(RESIDUAL_SCALE * first.astype(jnp.float32) + summed, norm_gain[1])
        return ffn_half(second, norm_gain[2])
    sequences = stream.reshape(SEQS, SEQLEN, D)
    return lax.map(one_sequence, sequences).reshape(TOKENS, D)
```

```python
import functools

import jax
import jax.numpy as jnp
import numpy as np
from jax import lax
from jax.experimental import pallas as pl
from jax.experimental.pallas import tpu as pltpu
from jax.sharding import PartitionSpec as P

DK = 64
DV = 128
RESIDUAL_SCALE = 2.0**0.5
BRANCH_SCALE = 0.5
NORM_EPS = 1e-05
HEAD_EPS = 0.01
GATE_DIVISOR = 16.0
MESH = pl.DeviceIdType.MESH
CUTS = 2
AHEAD = 2
HOST_AHEAD = 2
PARTS = 4
HOSTED = 4
F32 = jnp.float32
BF16 = jnp.bfloat16
NT = (((1,), (1,)), ((), ()))
TN = (((0,), (0,)), ((), ()))


def level_tables(tile):
    row, col = np.arange(tile)[:, None], np.arange(tile)[None, :]
    sums, pairs = [], []
    half = 1
    while half < tile:
        start = row // half * half
        later = row // half % 2 == 1
        sums.append(
            np.where(later, (col >= start) & (col <= row), (col > row) & (col < start + half))
        )
        pairs.append(later & (col // half == row // half - 1))
        half *= 2
    sums += [col <= row, col > row]
    pairs.append(row == col)
    return (
        np.concatenate(sums, 0).astype(np.float32),
        np.concatenate(pairs, 0).astype(np.float32),
        len(pairs) - 1,
    )


def dot(a, b, dims=None):
    if dims is None:
        return jnp.dot(a, b, preferred_element_type=F32)
    return lax.dot_general(a, b, dims, preferred_element_type=F32)


def layer_kernel(
    sizes,
    levels,
    cuts,
    stream,
    gate_w,
    up_w,
    down_w,
    qkvg_w,
    out_w,
    decay_down,
    decay_up,
    decay_bias,
    head_gain,
    norm_gain,
    span_sums,
    pair_masks,
    result,
    gate_all,
    up_all,
    down_all,
    qkvg_all,
    out_all,
    rows_all,
    part_out,
    part_in,
    cross_out,
    cross_in,
    partial,
    gate_buf,
    hidden,
    proj,
    log_gate,
    gated,
    state,
    guest_first,
    w_send,
    w_recv,
    ag_send,
    ag_recv,
    fwd_send,
    rs_send,
    rs_recv,
    cross_send,
    cross_recv,
    guest_send,
    guest_recv,
    home_send,
    home_recv,
):
    reps, shards, ranks, cores = sizes
    chips = ranks // cores
    rep, shard, rank = lax.axis_index("rep"), lax.axis_index("fs"), lax.axis_index("tp")
    chip, core = rank // cores, lax.rem(rank, cores)
    block, width = stream.shape
    length = block * ranks
    half_rows = chips * block
    partner = {"tp": chip * cores + (cores - 1 - core)}

    barrier = pltpu.get_barrier_semaphore()

    def greet(device):
        pl.semaphore_signal(barrier, inc=1, device_id=device, device_id_type=MESH)

    @pl.when(shard > 0)
    def _():
        greet({"fs": shard - 1})

    @pl.when(shard < shards - 1)
    def _():
        greet({"fs": shard + 1})

    for step in range(1, reps):
        greet({"rep": lax.rem(rep + step, reps)})
    for step in range(1, ranks):
        greet({"tp": lax.rem(rank + step, ranks)})
    neighbours = (
        jnp.where(shard > 0, 1, 0) + jnp.where(shard < shards - 1, 1, 0) + reps - 1 + ranks - 1
    )
    pl.semaphore_wait(barrier, neighbours)

    locals_ = (gate_w, up_w, down_w, qkvg_w, out_w)
    hosted = shards == HOSTED and cores > 1 and chips > 1
    guest = 3
    relayed = 3 * cuts
    items = len(locals_) * cuts
    direct = range(cuts // 2, 3 * cuts)
    at_end = (shard == 0) | (shard == shards - 1)
    at_host = jnp.logical_not(at_end)
    near = jnp.where(shard < shards // 2, 0, shards - 1)
    home = jnp.where(shard < shards // 2, 1, shards - 2)
    far_host = shards - 1 - shard

    def is_host(at):
        return (at > 0) & (at < shards - 1)

    wholes = (gate_all, up_all, down_all, qkvg_all, out_all)

    def side_by_side(w):
        return wholes[w].shape[0] == locals_[w].shape[0]

    def piece(item, owner, part):
        w, cut = item // cuts, item % cuts
        rows, columns = locals_[w].shape
        size = rows // (reps * cuts)
        start = (part * cuts + cut) * size
        if side_by_side(w):
            return wholes[w].at[
                pl.ds(pl.multiple_of(start, size), size),
                pl.ds(pl.multiple_of(owner * columns, columns), columns),
            ]
        return wholes[w].at[pl.ds(pl.multiple_of(owner * rows + start, size), size), :]

    def own_piece(item, part=rep):
        w, cut = item // cuts, item % cuts
        size = locals_[w].shape[0] // (reps * cuts)
        return locals_[w].at[pl.ds(pl.multiple_of((part * cuts + cut) * size, size), size), :]

    def weight_copy(w, owner, part, slot, device, source=None):
        target = piece(w, owner, part)
        return pltpu.make_async_remote_copy(
            src_ref=target if source is None else source,
            dst_ref=target,
            send_sem=w_send.at[w, owner, slot],
            recv_sem=w_recv.at[w, owner, part],
            device_id=device,
            device_id_type=MESH,
        )

    def own_right(w):
        return weight_copy(w, shard, rep, 0, {"fs": shard + 1}, own_piece(w))

    def own_left(w):
        return weight_copy(w, shard, rep, reps, {"fs": shard - 1}, own_piece(w))

    def send_own(w):
        @pl.when(shard < shards - 1)
        def _():
            own_right(w).start()

        @pl.when(shard > 0)
        def _():
            own_left(w).start()

    def own_to(item, toward):
        slot = jnp.where(toward > shard, 0, reps)
        return weight_copy(item, shard, rep, slot, {"fs": toward}, own_piece(item))

    def own_rest(item):
        copies = []
        for step in range(1, reps):
            part = lax.rem(rep + step, reps)
            source = own_piece(item, part)
            copies.append(weight_copy(item, shard, part, step, {"fs": home}, source))
        return copies

    def keep_own(w):
        rows, columns = locals_[w].shape
        if side_by_side(w):
            at = pl.ds(pl.multiple_of(shard * columns, columns), columns)
            wholes[w][:, at] = locals_[w][...]
        else:
            wholes[w][pl.ds(pl.multiple_of(shard * rows, rows), rows), :] = locals_[w][...]

    def others(body, nearest=1, furthest=shards - 1):
        def at_distance(d, carry):
            for sign in (-1, 1):
                owner = shard + sign * d

                @pl.when((owner >= 0) & (owner < shards))
                def _():
                    body(owner, shard - sign)

            return carry

        lax.fori_loop(nearest, furthest + 1, at_distance, 0)

    def onto(item, owner, onward):
        return weight_copy(item, owner, rep, 0, {"fs": onward})

    def sideways(item, owner):
        return [
            weight_copy(item, owner, rep, step, {"rep": lax.rem(rep + step, reps)})
            for step in range(1, reps)
        ]

    def relay(item, nearest=1, furthest=shards - 1):
        def body(owner, onward):
            weight_copy(item, owner, rep, 0, partner).wait_recv()

            @pl.when((onward >= 0) & (onward < shards))
            def _():
                onto(item, owner, onward).start()

            for copy in sideways(item, owner):
                copy.start()

        others(body, nearest, furthest)

    def relay_from(item, owner, onward):
        weight_copy(item, owner, rep, 0, partner).wait_recv()
        onto(item, owner, onward).start()
        for copy in sideways(item, owner):
            copy.start()

    def pass_on(item):
        weight_copy(item, near, rep, 0, partner).wait_recv()
        onto(item, near, far_host).start()
        if item not in direct:
            for copy in sideways(item, near):
                copy.start()
        if item + HOST_AHEAD < relayed:
            own_to(item + HOST_AHEAD, far_host).start()

    def pass_across(item, owner):
        weight_copy(item, owner, rep, 0, partner).wait_recv()
        for copy in sideways(item, owner):
            copy.start()

    def send_late(item):
        def body(owner, onward):
            @pl.when(jnp.logical_not(is_host(onward)))
            def _():
                onto(item, owner, onward).start()

        others(body)

    def arrive(w):
        def body(owner, onward):
            for step in range(1, reps):
                weight_copy(w, owner, lax.rem(rep + step, reps), step, partner).wait_recv()

        others(body)

    def arrive_from(item, owner):
        for step in range(1, reps):
            weight_copy(item, owner, lax.rem(rep + step, reps), step, partner).wait_recv()

    def drain(item):
        @pl.when(shard < shards - 1)
        def _():
            own_right(item).wait_send()

        @pl.when(shard > 0)
        def _():
            own_left(item).wait_send()

        first = hosted and item in direct
        if first:

            @pl.when(at_end)
            def _():
                for copy in own_rest(item):
                    copy.wait_send()

        def body(owner, onward):
            @pl.when((onward >= 0) & (onward < shards))
            def _():
                onto(item, owner, onward).wait_send()

            @pl.when(jnp.logical_not(first & at_host & is_host(onward)))
            def _():
                for copy in sideways(item, owner):
                    copy.wait_send()

        others(body)

    def position(chip_at, core_at):
        return pl.multiple_of((core_at * chips + chip_at) * block, block)

    strip = block // PARTS

    def row_copy(k, chip_at, core_at, send, part, device, source=None):
        at = pl.multiple_of(position(chip_at, core_at) + part * strip, strip)
        target = rows_all.at[k, pl.ds(at, strip), :]
        return pltpu.make_async_remote_copy(
            src_ref=target if source is None else source.at[pl.ds(part * strip, strip), :],
            dst_ref=target,
            send_sem=send.at[part],
            recv_sem=ag_recv.at[k, core_at * chips + chip_at, part],
            device_id=device,
            device_id_type=MESH,
        )

    def guest_copy(part):
        at = pl.multiple_of(position(chip, core) + part * strip, strip)
        return pltpu.make_async_remote_copy(
            src_ref=stream.at[pl.ds(part * strip, strip), :],
            dst_ref=rows_all.at[guest, pl.ds(at, strip), :],
            send_sem=guest_send.at[part],
            recv_sem=guest_recv.at[part],
            device_id={"fs": home},
            device_id_type=MESH,
        )

    def home_copy(part):
        at = pl.multiple_of(position(chip, core) + part * strip, strip)
        return pltpu.make_async_remote_copy(
            src_ref=guest_first.at[pl.ds(part * strip, strip), :],
            dst_ref=rows_all.at[1, pl.ds(at, strip), :],
            send_sem=home_send.at[part],
            recv_sem=home_recv.at[part],
            device_id={"fs": near},
            device_id_type=MESH,
        )

    def chip_away(step):
        return lax.rem(chip + step, chips)

    def gather_own(k, part, source):
        copies = []
        for step in range(1, chips):
            device = {"tp": chip_away(step) * cores + core}
            copies.append(row_copy(k, chip, core, ag_send.at[k, step], part, device, source))
        if cores > 1:
            copies.append(row_copy(k, chip, core, ag_send.at[k, 0], part, partner, source))
        return copies

    def forward(k, step, part):
        return row_copy(k, chip_away(step), core, fwd_send.at[k, step], part, partner)

    def mirrored(k, step, part):
        return row_copy(
            k, chip_away(step), cores - 1 - core, fwd_send.at[k, step], part, partner
        )

    def gather_start(k, part, source):
        for copy in gather_own(k, part, source):
            copy.start()

    def gathered(k, body):
        if cores > 1:
            for part in range(PARTS):
                mirrored(k, 0, part).wait_recv()

        def at_core(n, carry):
            body(pl.ds(position(chip, n), block))
            return carry

        lax.fori_loop(0, cores, at_core, 0)
        for step in range(1, chips):
            for part in range(PARTS):
                forward(k, step, part).wait_recv()
                if cores > 1:
                    forward(k, step, part).start()

            def at_turn(n, carry):
                @pl.when(n == 1)
                def _():
                    for part in range(PARTS):
                        mirrored(k, step, part).wait_recv()

                turn = jnp.where(n == 0, core, cores - 1 - core)
                body(pl.ds(position(chip_away(step), turn), block))
                return carry

            lax.fori_loop(0, cores, at_turn, 0)

    def part_copy(k, chip_at):
        rows = pl.ds(pl.multiple_of(chip_at * block, block), block)
        return pltpu.make_async_remote_copy(
            src_ref=part_out.at[k, rows, :],
            dst_ref=part_in.at[k, rows, :],
            send_sem=rs_send.at[k, chip_at, 0],
            recv_sem=rs_recv.at[k, lax.rem(chip_at - chip + chips, chips), 0],
            device_id=partner,
            device_id_type=MESH,
        )

    def cross_copy(k, step, part):
        rows = pl.ds(part * strip, strip)
        return pltpu.make_async_remote_copy(
            src_ref=cross_out.at[k, step - 1, rows, :],
            dst_ref=cross_in.at[k, step - 1, rows, :],
            send_sem=cross_send.at[k, step - 1, part],
            recv_sem=cross_recv.at[k, step - 1, part],
            device_id={"tp": chip_away(step) * cores + core},
            device_id_type=MESH,
        )

    def product(left, weights, core_at, chip_at, into):
        depth, columns = weights.shape[0] // shards, weights.shape[1]
        rows = left[pl.ds(position(chip_at, core_at), block), :]
        to = pl.ds(pl.multiple_of(chip_at * block, block), block)

        def at_shard(j, carry):
            value = dot(rows, weights[pl.ds(pl.multiple_of(j * depth, depth), depth), :])
            into[to, pl.ds(pl.multiple_of(j * columns, columns), columns)] = value.astype(
                into.dtype
            )
            return carry

        lax.fori_loop(0, shards, at_shard, 0)

    def reduce_start(k, left, weights):
        sums = partial.at[k // 3]

        for step in range(1, chips + 1):
            away = chip_away(step)
            if cores > 1:
                product(left, weights, cores - 1 - core, away, part_out.at[k])
                part_copy(k, away).start()
            product(left, weights, core, away, sums)
            if step < chips:
                if cores > 1:
                    part_copy(k, away).wait_recv()
                for part in range(PARTS):
                    rows = pl.ds(pl.multiple_of(away * block + part * strip, strip), strip)
                    value = sums[rows, :]
                    if cores > 1:
                        value = value + part_in[k, rows, :].astype(F32)
                    cross_out[k, step - 1, part * strip : (part + 1) * strip, :] = value.astype(
                        BF16
                    )
                    cross_copy(k, step, part).start()
        if cores > 1:
            part_copy(k, chip).wait_recv()

    depth, columns = locals_[2].shape

    def block_at(chip_at, j):
        return (
            pl.ds(pl.multiple_of(chip_at * block, block), block),
            pl.ds(pl.multiple_of(j * columns, columns), columns),
        )

    def part_block(k, chip_at, j):
        at = block_at(chip_at, j)
        return pltpu.make_async_remote_copy(
            src_ref=part_out.at[k, at[0], at[1]],
            dst_ref=part_in.at[k, at[0], at[1]],
            send_sem=rs_send.at[k, chip_at, j],
            recv_sem=rs_recv.at[k, lax.rem(chip_at - chip + chips, chips), j],
            device_id=partner,
            device_id_type=MESH,
        )

    def cross_block(k, step, j):
        at = block_at(0, j)[1]
        return pltpu.make_async_remote_copy(
            src_ref=cross_out.at[k, step - 1, :, at],
            dst_ref=cross_in.at[k, step - 1, :, at],
            send_sem=cross_send.at[k, step - 1, j],
            recv_sem=cross_recv.at[k, step - 1, j],
            device_id={"tp": chip_away(step) * cores + core},
            device_id_type=MESH,
        )

    def block_product(k, core_at, chip_at, j):
        rows = pl.ds(pl.multiple_of(k // 3 * length + position(chip_at, core_at), block), block)
        return dot(hidden[rows, :], down_all[pl.ds(pl.multiple_of(j * depth, depth), depth), :])

    def block_parts(k, chip_at, j):
        rows, at = block_at(chip_at, j)
        part_out[k, rows, at] = block_product(k, cores - 1 - core, chip_at, j).astype(BF16)
        part_block(k, chip_at, j).start()
        partial[k // 3, rows, at] = block_product(k, core, chip_at, j)

    def block_cross(k, j):
        for step in range(1, chips):
            away = chip_away(step)
            rows, at = block_at(away, j)
            part_block(k, away, j).wait_recv()
            value = partial[k // 3, rows, at] + part_in[k, rows, at].astype(F32)
            cross_out[k, step - 1, :, at] = value.astype(BF16)
            cross_block(k, step, j).start()

    def reduce_blocks(owners):
        for k in (guest, 0):
            for j in owners:
                for step in range(1, chips):
                    block_parts(k, chip_away(step), j)
            for j in owners:
                block_cross(k, j)

    def reduce_own(k):
        def at_shard(j, carry):
            block_parts(k, chip, j)
            return carry

        lax.fori_loop(0, shards, at_shard, 0)

    def blocks_landed(k):
        def at_shard(j, carry):
            part_block(k, chip, j).wait_recv()
            for step in range(1, chips):
                cross_block(k, step, j).wait_recv()
            return carry

        lax.fori_loop(0, shards, at_shard, 0)

    def drain_blocks(k):
        def at_shard(j, carry):
            for chip_at in range(chips):
                part_block(k, chip_at, j).wait_send()
            for step in range(1, chips):
                cross_block(k, step, j).wait_send()
            return carry

        lax.fori_loop(0, shards, at_shard, 0)

    chunk = min(32, block)

    def finish_norm(k, part, scale, branch, into, into_start, blocks=False):
        if not blocks:
            for step in range(1, chips):
                cross_copy(k, step, part).wait_recv()

        def at_chunk(n, carry):
            rows = pl.ds(pl.multiple_of(chip * block + n * chunk, chunk), chunk)
            inner = pl.ds(pl.multiple_of(n * chunk, chunk), chunk)
            summed = partial[k // 3, rows, :]
            if cores > 1:
                summed = summed + part_in[k, rows, :].astype(F32)
            for step in range(1, chips):
                summed = summed + cross_in[k, step - 1, inner, :].astype(F32)
            current = rows_all[
                k, pl.ds(pl.multiple_of(position(chip, core) + n * chunk, chunk), chunk), :
            ].astype(F32)
            values = RESIDUAL_SCALE * current + (summed if branch == 1.0 else branch * summed)
            centred = values - jnp.mean(values, -1, keepdims=True)
            spread = jnp.mean(centred * centred, -1, keepdims=True)
            done = (centred * lax.rsqrt(spread + NORM_EPS) * scale).astype(BF16)
            into[pl.ds(pl.multiple_of(into_start + n * chunk, chunk), chunk), :] = done
            return carry

        lax.fori_loop(part * strip // chunk, (part + 1) * strip // chunk, at_chunk, 0)

    def norm_to_rows(k, scale, branch, blocks=False):
        for part in range(PARTS):
            finish_norm(k, part, scale, branch, rows_all.at[k + 1], position(chip, core), blocks)
            gather_start(k + 1, part, None)

    high = min(256, length)

    def by_rows(body):
        def at_rows(m, carry):
            body(pl.ds(pl.multiple_of(m * high, high), high))
            return carry

        lax.fori_loop(0, length // high, at_rows, 0)

    def silu(values):
        return values / (1.0 + jnp.exp(-values))

    def shifted(rows, slot):
        return pl.ds(pl.multiple_of(rows.start + slot * length, high), high)

    def gate_rows(rows, k=0, slot=0):
        gate_buf[shifted(rows, slot), :] = silu(dot(rows_all[k, rows, :], gate_all[...], NT))

    def up_rows(rows, k=0, slot=0):
        upward = dot(rows_all[k, rows, :], up_all[...], NT)
        at = shifted(rows, slot)
        hidden[at, :] = (gate_buf[at, :] * upward).astype(BF16)

    def both(rows_body):
        by_rows(rows_body)
        by_rows(lambda rows: rows_body(rows, guest, 1))

    def hidden_rows(rows):
        upward = dot(rows_all[2, rows, :], up_all[...], NT)
        gate = silu(dot(rows_all[2, rows, :], gate_all[...], NT))
        hidden[rows, :] = (gate * upward).astype(BF16)

    keys = decay_up.shape[1]
    heads = keys // DK
    vals = heads * DV

    def project_rows(rows):
        first = rows_all[1, rows, :]
        low = dot(first, decay_down[...], NT).astype(BF16)
        pre = dot(low, decay_up[...]) + decay_bias[...]
        log_gate[rows, :] = (
            jnp.minimum(pre, 0.0) - jnp.log1p(jnp.exp(-jnp.abs(pre)))
        ) / GATE_DIVISOR
        proj[rows, :] = dot(first, qkvg_all[...]).astype(BF16)

    def mix():
        lane_head = lax.broadcasted_iota(jnp.int32, (1, keys), 1) // DK
        lane_masks = [jnp.where(lane_head == h, 1.0, 0.0) for h in range(heads)]
        state[...] = jnp.zeros_like(state)

        def at_tile(n, carry):
            rows = pl.ds(position(n // cores, lax.rem(n, cores)), block)
            query = proj[rows, 0:keys].astype(F32) * DK ** (-0.5)
            key_rows = proj[rows, keys : 2 * keys].astype(F32)
            value_rows = proj[rows, 2 * keys : 2 * keys + vals]
            decay = log_gate[rows, :]
            coarse = decay.astype(BF16)
            fine = (decay - coarse.astype(F32)).astype(BF16)

            def weight(at):
                table = span_sums[at * block : (at + 1) * block, :]
                return jnp.exp(dot(table, coarse) + dot(table, fine))

            scores = [jnp.zeros((block, block), F32) for _ in range(heads)]
            for at in range(levels + 1):
                pairs = pair_masks[at * block : (at + 1) * block, :]
                if at < levels:
                    factor = weight(at)
                    late, early = query * factor, (key_rows * factor).astype(BF16)
                else:
                    late, early = query, key_rows.astype(BF16)
                for h in range(heads):
                    scores[h] = scores[h] + pairs * dot(
                        (late * lane_masks[h]).astype(BF16), early, NT
                    )
            ahead = weight(levels)
            behind = weight(levels + 1)
            late = query * ahead
            held = state[...].astype(BF16)
            for h in range(heads):
                lanes = slice(h * DV, (h + 1) * DV)
                mixed = dot(scores[h].astype(BF16), value_rows[:, lanes]) + dot(
                    (late * lane_masks[h]).astype(BF16), held[lanes, :], NT
                )
                outgate = proj[
                    rows, 2 * keys + vals + h * DV : 2 * keys + vals + (h + 1) * DV
                ].astype(F32)
                normed = (
                    mixed
                    * lax.rsqrt(jnp.mean(mixed * mixed, -1, keepdims=True) + HEAD_EPS)
                    * head_gain[...]
                )
                gated[rows, lanes] = (normed * (outgate / (1.0 + jnp.exp(-outgate)))).astype(BF16)
            state[...] = state[...] * ahead[block - 1 : block, :] + dot(
                value_rows, (key_rows * behind).astype(BF16), TN
            )
            return carry

        lax.fori_loop(0, ranks, at_tile, 0)

    def pull(start, stop):
        for item in range(start, stop):
            relay(item)
            if item + AHEAD < items:
                send_own(item + AHEAD)

    def landed(w):
        for item in range(w * cuts, (w + 1) * cuts):
            arrive(item)

    own_at = pl.ds(position(chip, core), block)

    def opening():
        for item in range(min(AHEAD, items)):
            send_own(item)
        for part in range(PARTS):
            gather_start(0, part, stream)
        rows_all[0, own_at, :] = stream[...]
        for w in range(len(locals_)):
            keep_own(w)
        pull(0, cuts)
        gathered(0, lambda rows: None)
        pull(cuts, 2 * cuts)
        landed(0)
        by_rows(gate_rows)
        pull(2 * cuts, 3 * cuts)
        landed(1)
        by_rows(up_rows)
        pull(3 * cuts, 3 * cuts + cuts // 2)
        landed(2)
        reduce_start(0, hidden, down_all)
        pull(3 * cuts + cuts // 2, 4 * cuts)
        norm_to_rows(0, norm_gain[0:1, :], BRANCH_SCALE)
        pull(4 * cuts, 5 * cuts)

    def opening_host():
        for item in range(min(HOST_AHEAD, relayed)):
            own_to(item, far_host).start()
        for part in range(PARTS):
            gather_start(0, part, stream)
        for item in range(relayed, items):
            own_to(item, near).start()
        for item in range(relayed):
            own_to(item, near).start()
        rows_all[0, own_at, :] = stream[...]
        for w in range(len(locals_)):
            keep_own(w)
        far_end = shards - 1 - near
        gates, ups, downs = (range(w * cuts, (w + 1) * cuts) for w in range(3))
        for item in gates:
            pass_on(item)
        for item in gates:
            pass_across(item, far_host)
            pass_across(item, far_end)
        for item in gates:
            send_late(item)
        for part in range(PARTS):
            guest_copy(part).wait_recv()
            gather_start(guest, part, None)
        for item in ups:
            pass_on(item)
            pass_across(item, far_host)
            if item == cuts:
                gathered(0, lambda rows: None)
            pass_across(item, far_end)
        for item in ups:
            onto(item, far_host, near).start()
        for item in downs:
            pass_on(item)
            pass_across(item, far_host)
        for item in range(relayed, items):
            own_to(item, far_host).start()
        gathered(guest, lambda rows: None)
        landed(0)
        both(gate_rows)
        landed(1)
        both(up_rows)
        pass_across(2 * cuts, far_end)
        reduce_blocks([shard])
        for item in downs[1:]:
            pass_across(item, far_end)
        down_items = range(2 * cuts, 3 * cuts)
        qkvg_items = range(3 * cuts, 4 * cuts)
        out_items = range(4 * cuts, 5 * cuts)
        for item in down_items:
            arrive_from(item, near)
        reduce_blocks([near])
        for item in qkvg_items:
            relay_from(item, far_host, near)
        for item in down_items:
            arrive_from(item, far_host)
            arrive_from(item, far_end)
        reduce_blocks([far_host, far_end])
        for item in qkvg_items:
            relay_from(item, near, far_host)
        reduce_own(guest)
        reduce_own(0)
        blocks_landed(guest)
        for part in range(PARTS):
            finish_norm(guest, part, norm_gain[0:1, :], BRANCH_SCALE, guest_first, 0, True)
            home_copy(part).start()
        for item in qkvg_items:
            relay_from(item, far_end, near)
        for item in out_items:
            relay_from(item, near, far_host)
            relay_from(item, far_host, near)
        blocks_landed(0)
        norm_to_rows(0, norm_gain[0:1, :], BRANCH_SCALE, True)
        for item in out_items:
            relay_from(item, far_end, near)
        for item in ups:
            onto(item, far_end, near).start()
        for item in downs:
            send_late(item)

    def opening_end():
        for item in range(cuts):
            own_to(item, home).start()
        for part in range(PARTS):
            guest_copy(part).start()
        for w in range(3):
            if w < 2:
                for item in range((w + 1) * cuts, (w + 2) * cuts):
                    own_to(item, home).start()
            for item in range(w * cuts, (w + 1) * cuts):
                if item in direct:
                    for copy in own_rest(item):
                        copy.start()
        for item in range(relayed, items):
            own_to(item, home).start()
        for w in range(len(locals_)):
            keep_own(w)
        for item in range(relayed, items):
            relay(item, 1, 1)
        for item in range(relayed):
            relay(item, 1, 1)
        for item in range(cuts):
            relay(item, 2)
        for item in range(cuts, 2 * cuts):
            relay(item, 2, 2)
        for item in range(relayed, 4 * cuts):
            relay(item, 2, 2)
        for part in range(PARTS):
            home_copy(part).wait_recv()
            gather_start(1, part, None)
        for item in range(relayed, 4 * cuts):
            relay(item, 3)
        for item in range(4 * cuts, items):
            relay(item, 2)

    def late(start, stop, nearest=2):
        if hosted:

            @pl.when(at_end)
            def _():
                for item in range(start, stop):
                    relay(item, nearest)

    def late_landed(w):
        if hosted:

            @pl.when(at_end)
            def _():
                landed(w)

    if hosted:
        pl.when(at_host)(opening_host)
        pl.when(at_end)(opening_end)
    else:
        opening()
    landed(3)
    gathered(1, project_rows)
    mix()
    late(cuts, 2 * cuts, 3)
    landed(4)
    reduce_start(1, gated, out_all)
    late(2 * cuts, 2 * cuts + 1)
    norm_to_rows(1, norm_gain[1:2, :], 1.0)
    late(2 * cuts + 1, 3 * cuts)
    late_landed(0)
    late_landed(1)
    gathered(2, hidden_rows)
    late_landed(2)
    reduce_start(2, hidden, down_all)
    for part in range(PARTS):
        finish_norm(2, part, norm_gain[2:3, :], BRANCH_SCALE, result, 0)

    for item in range(items):
        drain(item)

    def drain_rows(k, source=None):
        for part in range(PARTS):
            for copy in gather_own(k, part, source):
                copy.wait_send()
            for step in range(1, chips):
                if cores > 1:
                    forward(k, step, part).wait_send()

    def drain_sums(k):
        for part in range(PARTS):
            for step in range(1, chips):
                cross_copy(k, step, part).wait_send()
        if cores > 1:
            for chip_at in range(chips):
                part_copy(k, chip_at).wait_send()

    def drain_host():
        drain_rows(guest)
        drain_blocks(guest)
        for part in range(PARTS):
            home_copy(part).wait_send()

    def drain_end():
        for part in range(PARTS):
            guest_copy(part).wait_send()

    def drain_opening():
        drain_rows(0, stream)
        if hosted:
            drain_blocks(0)
        else:
            drain_sums(0)

    if hosted:

        @pl.when(at_host)
        def _():
            drain_opening()
            drain_host()

        pl.when(at_end)(drain_end)
    else:
        drain_opening()
    for k in (1, 2):
        drain_rows(k)
        drain_sums(k)


def solution(mesh):
    reps, shards, ranks = mesh.shape["rep"], mesh.shape["fs"], mesh.shape["tp"]
    cores = 2 if ranks % 2 == 0 else 1
    chips = ranks // cores

    def on_device(
        stream,
        gate_weight,
        up_weight,
        down_weight,
        query_weight,
        key_weight,
        value_weight,
        outgate_weight,
        decay_down,
        decay_up,
        decay_bias,
        head_gain,
        out_weight,
        norm_gain,
    ):
        qkvg = jnp.concatenate([query_weight, key_weight, value_weight, outgate_weight], axis=1)
        block, width = stream.shape
        length, half_rows = block * ranks, block * chips
        hidden_width = gate_weight.shape[1]
        keys = decay_up.shape[1]
        vals = value_weight.shape[1]
        sums, pairs, levels = level_tables(block)
        vmem = pl.BlockSpec(memory_space=pltpu.VMEM)
        away = max(chips - 1, 1)
        hosted = shards == HOSTED and cores > 1 and chips > 1
        phases, slots = (4, 2) if hosted else (3, 1)
        weights = (gate_weight.T, up_weight.T, down_weight, qkvg, out_weight)
        dma = pltpu.SemaphoreType.DMA
        cuts = max(c for c in (1, CUTS) if all(w.shape[0] % (16 * reps * c) == 0 for w in weights))
        return pl.pallas_call(
            functools.partial(layer_kernel, (reps, shards, ranks, cores), levels, cuts),
            out_shape=jax.ShapeDtypeStruct((block, width), BF16),
            in_specs=[vmem] * 13,
            out_specs=vmem,
            scratch_shapes=[
                *[pltpu.VMEM((w.shape[0], shards * w.shape[1]), BF16) for w in weights[:2]],
                *[pltpu.VMEM((shards * w.shape[0], w.shape[1]), BF16) for w in weights[2:]],
                pltpu.VMEM((phases, length, width), BF16),
                pltpu.VMEM((phases, half_rows, width), BF16),
                pltpu.VMEM((phases, half_rows, width), BF16),
                pltpu.VMEM((phases, away, block, width), BF16),
                pltpu.VMEM((phases, away, block, width), BF16),
                pltpu.VMEM((slots, half_rows, width), F32),
                pltpu.VMEM((slots * length, hidden_width), F32),
                pltpu.VMEM((slots * length, hidden_width), BF16),
                pltpu.VMEM((length, qkvg.shape[1]), BF16),
                pltpu.VMEM((length, keys), F32),
                pltpu.VMEM((length, vals), BF16),
                pltpu.VMEM((vals, keys), F32),
                pltpu.VMEM((block, width), BF16),
                dma((5 * cuts, shards, reps + 1)),
                dma((5 * cuts, shards, reps)),
                dma((phases, chips, PARTS)),
                dma((phases, ranks, PARTS)),
                dma((phases, chips, PARTS)),
                dma((phases, chips, shards)),
                dma((phases, chips, shards)),
                dma((phases, away, max(PARTS, shards))),
                dma((phases, away, max(PARTS, shards))),
                *[dma((PARTS,))] * 4,
            ],
            compiler_params=pltpu.CompilerParams(
                collective_id=0, has_side_effects=True, vmem_limit_bytes=60 * 2**20
            ),
            name="layer",
        )(
            stream,
            *weights,
            decay_down.T,
            decay_up,
            decay_bias[None, :],
            head_gain[None, :],
            norm_gain,
            jnp.asarray(sums, BF16),
            jnp.asarray(pairs, F32),
        )

    in_specs = (
        P(("rep", "fs", "tp"), None),
        P("fs", "tp"),
        P("fs", "tp"),
        P("tp", "fs"),
        P("fs", "tp"),
        P("fs", "tp"),
        P("fs", "tp"),
        P("fs", "tp"),
        P(),
        P(None, "tp"),
        P("tp"),
        P(),
        P("tp", "fs"),
        P(),
    )
    return jax.shard_map(
        on_device,
        mesh=mesh,
        in_specs=in_specs,
        out_specs=P(("rep", "fs", "tp"), None),
        check_vma=False,
    )
```

```python
import functools

import jax
import jax.numpy as jnp
import numpy as np
from jax import lax
from jax.experimental import pallas as pl
from jax.experimental.pallas import tpu as pltpu
from jax.sharding import PartitionSpec as P

DK = 64
DV = 128
RESIDUAL_SCALE = 2.0**0.5
BRANCH_SCALE = 0.5
NORM_EPS = 1e-05
HEAD_EPS = 0.01
GATE_DIVISOR = 16.0
MESH = pl.DeviceIdType.MESH
CUTS = 2
AHEAD = 2
HOST_AHEAD = 2
PARTS = 4
HOSTED = 4
F32 = jnp.float32
BF16 = jnp.bfloat16
NT = (((1,), (1,)), ((), ()))
TN = (((0,), (0,)), ((), ()))


def level_tables(tile):
    row, col = np.arange(tile)[:, None], np.arange(tile)[None, :]
    sums, pairs = [], []
    half = 1
    while half < tile:
        start = row // half * half
        later = row // half % 2 == 1
        sums.append(
            np.where(later, (col >= start) & (col <= row), (col > row) & (col < start + half))
        )
        pairs.append(later & (col // half == row // half - 1))
        half *= 2
    sums += [col <= row, col > row]
    pairs.append(row == col)
    return (
        np.concatenate(sums, 0).astype(np.float32),
        np.concatenate(pairs, 0).astype(np.float32),
        len(pairs) - 1,
    )


def dot(a, b, dims=None):
    if dims is None:
        return jnp.dot(a, b, preferred_element_type=F32)
    return lax.dot_general(a, b, dims, preferred_element_type=F32)


def layer_kernel(
    sizes,
    levels,
    cuts,
    stream,
    gate_w,
    up_w,
    down_w,
    query_w,
    key_w,
    value_w,
    outgate_w,
    out_w,
    decay_down,
    decay_up,
    decay_bias,
    head_gain,
    norm_gain,
    span_sums,
    pair_masks,
    result,
    gate_all,
    up_all,
    down_all,
    qkvg_all,
    out_all,
    rows_all,
    part_out,
    part_in,
    cross_out,
    cross_in,
    partial,
    gate_buf,
    hidden,
    proj,
    log_gate,
    gated,
    state,
    guest_first,
    qkvg_w,
    proj_sums,
    w_send,
    w_recv,
    ag_send,
    ag_recv,
    fwd_send,
    rs_send,
    rs_recv,
    cross_send,
    cross_recv,
    guest_send,
    guest_recv,
    home_send,
    home_recv,
):
    reps, shards, ranks, cores = sizes
    chips = ranks // cores
    rep, shard, rank = lax.axis_index("rep"), lax.axis_index("fs"), lax.axis_index("tp")
    chip, core = rank // cores, lax.rem(rank, cores)
    block, width = stream.shape
    length = block * ranks
    half_rows = chips * block
    partner = {"tp": chip * cores + (cores - 1 - core)}

    barrier = pltpu.get_barrier_semaphore()

    def greet(device):
        pl.semaphore_signal(barrier, inc=1, device_id=device, device_id_type=MESH)

    @pl.when(shard > 0)
    def _():
        greet({"fs": shard - 1})

    @pl.when(shard < shards - 1)
    def _():
        greet({"fs": shard + 1})

    for step in range(1, reps):
        greet({"rep": lax.rem(rep + step, reps)})
    for step in range(1, ranks):
        greet({"tp": lax.rem(rank + step, ranks)})
    neighbours = (
        jnp.where(shard > 0, 1, 0) + jnp.where(shard < shards - 1, 1, 0) + reps - 1 + ranks - 1
    )
    pl.semaphore_wait(barrier, neighbours)

    lane = 0
    for w in (query_w, key_w, value_w, outgate_w):
        qkvg_w[:, lane : lane + w.shape[1]] = w[...]
        lane += w.shape[1]

    locals_ = (gate_w, up_w, down_w, qkvg_w, out_w)
    hosted = shards == HOSTED and cores > 1 and chips > 1
    guest = 3
    relayed = 3 * cuts
    items = len(locals_) * cuts
    direct = range(cuts // 2, 3 * cuts)
    at_end = (shard == 0) | (shard == shards - 1)
    at_host = jnp.logical_not(at_end)
    near = jnp.where(shard < shards // 2, 0, shards - 1)
    home = jnp.where(shard < shards // 2, 1, shards - 2)
    far_host = shards - 1 - shard

    def is_host(at):
        return (at > 0) & (at < shards - 1)

    wholes = (gate_all, up_all, down_all, qkvg_all, out_all)

    def side_by_side(w):
        return wholes[w].shape[0] == locals_[w].shape[0]

    def piece(item, owner, part):
        w, cut = item // cuts, item % cuts
        rows, columns = locals_[w].shape
        size = rows // (reps * cuts)
        start = (part * cuts + cut) * size
        if side_by_side(w):
            return wholes[w].at[
                pl.ds(pl.multiple_of(start, size), size),
                pl.ds(pl.multiple_of(owner * columns, columns), columns),
            ]
        return wholes[w].at[pl.ds(pl.multiple_of(owner * rows + start, size), size), :]

    def own_piece(item, part=rep):
        w, cut = item // cuts, item % cuts
        size = locals_[w].shape[0] // (reps * cuts)
        return locals_[w].at[pl.ds(pl.multiple_of((part * cuts + cut) * size, size), size), :]

    def weight_copy(w, owner, part, slot, device, source=None):
        target = piece(w, owner, part)
        return pltpu.make_async_remote_copy(
            src_ref=target if source is None else source,
            dst_ref=target,
            send_sem=w_send.at[w, owner, slot],
            recv_sem=w_recv.at[w, owner, part],
            device_id=device,
            device_id_type=MESH,
        )

    def own_right(w):
        return weight_copy(w, shard, rep, 0, {"fs": shard + 1}, own_piece(w))

    def own_left(w):
        return weight_copy(w, shard, rep, reps, {"fs": shard - 1}, own_piece(w))

    def send_own(w):
        @pl.when(shard < shards - 1)
        def _():
            own_right(w).start()

        @pl.when(shard > 0)
        def _():
            own_left(w).start()

    def own_to(item, toward):
        slot = jnp.where(toward > shard, 0, reps)
        return weight_copy(item, shard, rep, slot, {"fs": toward}, own_piece(item))

    def own_rest(item):
        copies = []
        for step in range(1, reps):
            part = lax.rem(rep + step, reps)
            source = own_piece(item, part)
            copies.append(weight_copy(item, shard, part, step, {"fs": home}, source))
        return copies

    def keep_own(w):
        rows, columns = locals_[w].shape
        if side_by_side(w):
            at = pl.ds(pl.multiple_of(shard * columns, columns), columns)
            wholes[w][:, at] = locals_[w][...]
        else:
            wholes[w][pl.ds(pl.multiple_of(shard * rows, rows), rows), :] = locals_[w][...]

    def others(body, nearest=1, furthest=shards - 1):
        def at_distance(d, carry):
            for sign in (-1, 1):
                owner = shard + sign * d

                @pl.when((owner >= 0) & (owner < shards))
                def _():
                    body(owner, shard - sign)

            return carry

        lax.fori_loop(nearest, furthest + 1, at_distance, 0)

    def onto(item, owner, onward):
        return weight_copy(item, owner, rep, 0, {"fs": onward})

    def sideways(item, owner):
        return [
            weight_copy(item, owner, rep, step, {"rep": lax.rem(rep + step, reps)})
            for step in range(1, reps)
        ]

    def relay(item, nearest=1, furthest=shards - 1):
        def body(owner, onward):
            weight_copy(item, owner, rep, 0, partner).wait_recv()

            @pl.when((onward >= 0) & (onward < shards))
            def _():
                onto(item, owner, onward).start()

            for copy in sideways(item, owner):
                copy.start()

        others(body, nearest, furthest)

    def relay_from(item, owner, onward):
        weight_copy(item, owner, rep, 0, partner).wait_recv()
        onto(item, owner, onward).start()
        for copy in sideways(item, owner):
            copy.start()

    def pass_on(item):
        weight_copy(item, near, rep, 0, partner).wait_recv()
        onto(item, near, far_host).start()
        if item not in direct:
            for copy in sideways(item, near):
                copy.start()
        if item + HOST_AHEAD < relayed:
            own_to(item + HOST_AHEAD, far_host).start()

    def pass_across(item, owner):
        weight_copy(item, owner, rep, 0, partner).wait_recv()
        for copy in sideways(item, owner):
            copy.start()

    def send_late(item):
        def body(owner, onward):
            @pl.when(jnp.logical_not(is_host(onward)))
            def _():
                onto(item, owner, onward).start()

        others(body)

    def arrive(w):
        def body(owner, onward):
            for step in range(1, reps):
                weight_copy(w, owner, lax.rem(rep + step, reps), step, partner).wait_recv()

        others(body)

    def arrive_from(item, owner):
        for step in range(1, reps):
            weight_copy(item, owner, lax.rem(rep + step, reps), step, partner).wait_recv()

    def drain(item):
        @pl.when(shard < shards - 1)
        def _():
            own_right(item).wait_send()

        @pl.when(shard > 0)
        def _():
            own_left(item).wait_send()

        first = hosted and item in direct
        if first:

            @pl.when(at_end)
            def _():
                for copy in own_rest(item):
                    copy.wait_send()

        def body(owner, onward):
            @pl.when((onward >= 0) & (onward < shards))
            def _():
                onto(item, owner, onward).wait_send()

            @pl.when(jnp.logical_not(first & at_host & is_host(onward)))
            def _():
                for copy in sideways(item, owner):
                    copy.wait_send()

        others(body)

    def position(chip_at, core_at):
        return pl.multiple_of((core_at * chips + chip_at) * block, block)

    strip = block // PARTS

    def row_copy(k, chip_at, core_at, send, part, device, source=None):
        at = pl.multiple_of(position(chip_at, core_at) + part * strip, strip)
        target = rows_all.at[k, pl.ds(at, strip), :]
        return pltpu.make_async_remote_copy(
            src_ref=target if source is None else source.at[pl.ds(part * strip, strip), :],
            dst_ref=target,
            send_sem=send.at[part],
            recv_sem=ag_recv.at[k, core_at * chips + chip_at, part],
            device_id=device,
            device_id_type=MESH,
        )

    def guest_copy(part):
        at = pl.multiple_of(position(chip, core) + part * strip, strip)
        return pltpu.make_async_remote_copy(
            src_ref=stream.at[pl.ds(part * strip, strip), :],
            dst_ref=rows_all.at[guest, pl.ds(at, strip), :],
            send_sem=guest_send.at[part],
            recv_sem=guest_recv.at[part],
            device_id={"fs": home},
            device_id_type=MESH,
        )

    def home_copy(part):
        at = pl.multiple_of(position(chip, core) + part * strip, strip)
        return pltpu.make_async_remote_copy(
            src_ref=guest_first.at[pl.ds(part * strip, strip), :],
            dst_ref=rows_all.at[1, pl.ds(at, strip), :],
            send_sem=home_send.at[part],
            recv_sem=home_recv.at[part],
            device_id={"fs": near},
            device_id_type=MESH,
        )

    def chip_away(step):
        return lax.rem(chip + step, chips)

    def gather_own(k, part, source):
        copies = []
        for step in range(1, chips):
            device = {"tp": chip_away(step) * cores + core}
            copies.append(row_copy(k, chip, core, ag_send.at[k, step], part, device, source))
        if cores > 1:
            copies.append(row_copy(k, chip, core, ag_send.at[k, 0], part, partner, source))
        return copies

    def forward(k, step, part):
        return row_copy(k, chip_away(step), core, fwd_send.at[k, step], part, partner)

    def mirrored(k, step, part):
        return row_copy(
            k, chip_away(step), cores - 1 - core, fwd_send.at[k, step], part, partner
        )

    def gather_start(k, part, source):
        for copy in gather_own(k, part, source):
            copy.start()

    def gathered(k, body):
        if cores > 1:
            for part in range(PARTS):
                mirrored(k, 0, part).wait_recv()

        def at_core(n, carry):
            body(pl.ds(position(chip, n), block))
            return carry

        lax.fori_loop(0, cores, at_core, 0)
        for step in range(1, chips):
            for part in range(PARTS):
                forward(k, step, part).wait_recv()
                if cores > 1:
                    forward(k, step, part).start()

            def at_turn(n, carry):
                @pl.when(n == 1)
                def _():
                    for part in range(PARTS):
                        mirrored(k, step, part).wait_recv()

                turn = jnp.where(n == 0, core, cores - 1 - core)
                body(pl.ds(position(chip_away(step), turn), block))
                return carry

            lax.fori_loop(0, cores, at_turn, 0)

    def part_copy(k, chip_at):
        rows = pl.ds(pl.multiple_of(chip_at * block, block), block)
        return pltpu.make_async_remote_copy(
            src_ref=part_out.at[k, rows, :],
            dst_ref=part_in.at[k, rows, :],
            send_sem=rs_send.at[k, chip_at, 0],
            recv_sem=rs_recv.at[k, lax.rem(chip_at - chip + chips, chips), 0],
            device_id=partner,
            device_id_type=MESH,
        )

    def cross_copy(k, step, part):
        rows = pl.ds(part * strip, strip)
        return pltpu.make_async_remote_copy(
            src_ref=cross_out.at[k, step - 1, rows, :],
            dst_ref=cross_in.at[k, step - 1, rows, :],
            send_sem=cross_send.at[k, step - 1, part],
            recv_sem=cross_recv.at[k, step - 1, part],
            device_id={"tp": chip_away(step) * cores + core},
            device_id_type=MESH,
        )

    def product(left, weights, core_at, chip_at, into):
        depth, columns = weights.shape[0] // shards, weights.shape[1]
        rows = left[pl.ds(position(chip_at, core_at), block), :]
        to = pl.ds(pl.multiple_of(chip_at * block, block), block)

        def at_shard(j, carry):
            value = dot(rows, weights[pl.ds(pl.multiple_of(j * depth, depth), depth), :])
            into[to, pl.ds(pl.multiple_of(j * columns, columns), columns)] = value.astype(
                into.dtype
            )
            return carry

        lax.fori_loop(0, shards, at_shard, 0)

    def reduce_start(k, left, weights):
        sums = partial.at[k // 3]

        for step in range(1, chips + 1):
            away = chip_away(step)
            if cores > 1:
                product(left, weights, cores - 1 - core, away, part_out.at[k])
                part_copy(k, away).start()
            product(left, weights, core, away, sums)
            if step < chips:
                if cores > 1:
                    part_copy(k, away).wait_recv()
                for part in range(PARTS):
                    rows = pl.ds(pl.multiple_of(away * block + part * strip, strip), strip)
                    value = sums[rows, :]
                    if cores > 1:
                        value = value + part_in[k, rows, :].astype(F32)
                    cross_out[k, step - 1, part * strip : (part + 1) * strip, :] = value.astype(
                        BF16
                    )
                    cross_copy(k, step, part).start()
        if cores > 1:
            part_copy(k, chip).wait_recv()

    depth, columns = locals_[2].shape

    def block_at(chip_at, j):
        return (
            pl.ds(pl.multiple_of(chip_at * block, block), block),
            pl.ds(pl.multiple_of(j * columns, columns), columns),
        )

    def part_block(k, chip_at, j):
        at = block_at(chip_at, j)
        return pltpu.make_async_remote_copy(
            src_ref=part_out.at[k, at[0], at[1]],
            dst_ref=part_in.at[k, at[0], at[1]],
            send_sem=rs_send.at[k, chip_at, j],
            recv_sem=rs_recv.at[k, lax.rem(chip_at - chip + chips, chips), j],
            device_id=partner,
            device_id_type=MESH,
        )

    def cross_block(k, step, j):
        at = block_at(0, j)[1]
        return pltpu.make_async_remote_copy(
            src_ref=cross_out.at[k, step - 1, :, at],
            dst_ref=cross_in.at[k, step - 1, :, at],
            send_sem=cross_send.at[k, step - 1, j],
            recv_sem=cross_recv.at[k, step - 1, j],
            device_id={"tp": chip_away(step) * cores + core},
            device_id_type=MESH,
        )

    def block_product(k, core_at, chip_at, j):
        rows = pl.ds(pl.multiple_of(k // 3 * length + position(chip_at, core_at), block), block)
        return dot(hidden[rows, :], down_all[pl.ds(pl.multiple_of(j * depth, depth), depth), :])

    def block_parts(k, chip_at, j):
        rows, at = block_at(chip_at, j)
        part_out[k, rows, at] = block_product(k, cores - 1 - core, chip_at, j).astype(BF16)
        part_block(k, chip_at, j).start()
        partial[k // 3, rows, at] = block_product(k, core, chip_at, j)

    def block_cross(k, j):
        for step in range(1, chips):
            away = chip_away(step)
            rows, at = block_at(away, j)
            part_block(k, away, j).wait_recv()
            value = partial[k // 3, rows, at] + part_in[k, rows, at].astype(F32)
            cross_out[k, step - 1, :, at] = value.astype(BF16)
            cross_block(k, step, j).start()

    def reduce_blocks(owners):
        for k in (guest, 0):
            for j in owners:
                for step in range(1, chips):
                    block_parts(k, chip_away(step), j)
            if k == guest:
                for j in owners:
                    block_cross(k, j)

    def reduce_own(k):
        def at_shard(j, carry):
            block_parts(k, chip, j)
            return carry

        lax.fori_loop(0, shards, at_shard, 0)

    def blocks_landed(k):
        def at_shard(j, carry):
            part_block(k, chip, j).wait_recv()
            for step in range(1, chips):
                cross_block(k, step, j).wait_recv()
            return carry

        lax.fori_loop(0, shards, at_shard, 0)

    def drain_blocks(k):
        def at_shard(j, carry):
            for chip_at in range(chips):
                part_block(k, chip_at, j).wait_send()
            for step in range(1, chips):
                cross_block(k, step, j).wait_send()
            return carry

        lax.fori_loop(0, shards, at_shard, 0)

    chunk = min(32, strip)

    def finish_norm(k, part, scale, branch, into, into_start, blocks=False):
        if not blocks:
            for step in range(1, chips):
                cross_copy(k, step, part).wait_recv()

        def at_chunk(n, carry):
            rows = pl.ds(pl.multiple_of(chip * block + n * chunk, chunk), chunk)
            inner = pl.ds(pl.multiple_of(n * chunk, chunk), chunk)
            summed = partial[k // 3, rows, :]
            if cores > 1:
                summed = summed + part_in[k, rows, :].astype(F32)
            for step in range(1, chips):
                summed = summed + cross_in[k, step - 1, inner, :].astype(F32)
            current = rows_all[
                k, pl.ds(pl.multiple_of(position(chip, core) + n * chunk, chunk), chunk), :
            ].astype(F32)
            values = RESIDUAL_SCALE * current + (summed if branch == 1.0 else branch * summed)
            centred = values - jnp.mean(values, -1, keepdims=True)
            spread = jnp.mean(centred * centred, -1, keepdims=True)
            done = (centred * lax.rsqrt(spread + NORM_EPS) * scale).astype(BF16)
            into[pl.ds(pl.multiple_of(into_start + n * chunk, chunk), chunk), :] = done
            return carry

        lax.fori_loop(part * strip // chunk, (part + 1) * strip // chunk, at_chunk, 0)

    def norm_to_rows(k, scale, branch, blocks=False):
        for part in range(PARTS):
            finish_norm(k, part, scale, branch, rows_all.at[k + 1], position(chip, core), blocks)
            gather_start(k + 1, part, None)

    high = min(256, length)

    def by_rows(body):
        def at_rows(m, carry):
            body(pl.ds(pl.multiple_of(m * high, high), high))
            return carry

        lax.fori_loop(0, length // high, at_rows, 0)

    def silu(values):
        return values / (1.0 + jnp.exp(-values))

    def shifted(rows, slot):
        return pl.ds(pl.multiple_of(rows.start + slot * length, high), high)

    def gate_rows(rows, k=0, slot=0):
        gate_buf[shifted(rows, slot), :] = silu(dot(rows_all[k, rows, :], gate_all[...], NT))

    def up_rows(rows, k=0, slot=0):
        upward = dot(rows_all[k, rows, :], up_all[...], NT)
        at = shifted(rows, slot)
        hidden[at, :] = (gate_buf[at, :] * upward).astype(BF16)

    def both(rows_body):
        by_rows(rows_body)
        by_rows(lambda rows: rows_body(rows, guest, 1))

    def hidden_rows(rows):
        upward = dot(rows_all[2, rows, :], up_all[...], NT)
        gate = silu(dot(rows_all[2, rows, :], gate_all[...], NT))
        hidden[rows, :] = (gate * upward).astype(BF16)

    keys = decay_up.shape[1]
    heads = keys // DK
    vals = heads * DV

    furthest = jnp.where(at_end, shards - 1 - shard, shards - 1 - near)

    def slab(rows, j):
        deep = qkvg_w.shape[0]
        at = pl.ds(pl.multiple_of(j * deep, deep), deep)
        return dot(rows_all[1, rows, at], qkvg_all[at, :])

    def project_most(rows):
        decay_rows(rows)
        total = slab(rows, lax.rem(furthest + 1, shards))
        for step in range(2, shards):
            total = total + slab(rows, lax.rem(furthest + step, shards))
        proj_sums[rows, :] = total

    def project_last(rows):
        proj[rows, :] = (proj_sums[rows, :] + slab(rows, furthest)).astype(BF16)

    def project_rows(rows):
        decay_rows(rows)
        proj[rows, :] = dot(rows_all[1, rows, :], qkvg_all[...]).astype(BF16)

    def decay_rows(rows):
        low = dot(rows_all[1, rows, :], decay_down[...], NT).astype(BF16)
        pre = dot(low, decay_up[...]) + decay_bias[...]
        log_gate[rows, :] = (
            jnp.minimum(pre, 0.0) - jnp.log1p(jnp.exp(-jnp.abs(pre)))
        ) / GATE_DIVISOR

    def mix():
        lane_head = lax.broadcasted_iota(jnp.int32, (1, keys), 1) // DK
        lane_masks = [jnp.where(lane_head == h, 1.0, 0.0) for h in range(heads)]
        state[...] = jnp.zeros_like(state)

        def at_tile(n, carry):
            rows = pl.ds(position(n // cores, lax.rem(n, cores)), block)
            query = proj[rows, 0:keys].astype(F32) * DK ** (-0.5)
            key_rows = proj[rows, keys : 2 * keys].astype(F32)
            value_rows = proj[rows, 2 * keys : 2 * keys + vals]
            decay = log_gate[rows, :]
            coarse = decay.astype(BF16)
            fine = (decay - coarse.astype(F32)).astype(BF16)

            def weight(at):
                table = span_sums[at * block : (at + 1) * block, :]
                return jnp.exp(dot(table, coarse) + dot(table, fine))

            scores = [jnp.zeros((block, block), F32) for _ in range(heads)]
            for at in range(levels + 1):
                pairs = pair_masks[at * block : (at + 1) * block, :]
                if at < levels:
                    factor = weight(at)
                    late, early = query * factor, (key_rows * factor).astype(BF16)
                else:
                    late, early = query, key_rows.astype(BF16)
                for h in range(heads):
                    scores[h] = scores[h] + pairs * dot(
                        (late * lane_masks[h]).astype(BF16), early, NT
                    )
            ahead = weight(levels)
            behind = weight(levels + 1)
            late = query * ahead
            held = state[...].astype(BF16)
            for h in range(heads):
                lanes = slice(h * DV, (h + 1) * DV)
                mixed = dot(scores[h].astype(BF16), value_rows[:, lanes]) + dot(
                    (late * lane_masks[h]).astype(BF16), held[lanes, :], NT
                )
                outgate = proj[
                    rows, 2 * keys + vals + h * DV : 2 * keys + vals + (h + 1) * DV
                ].astype(F32)
                normed = (
                    mixed
                    * lax.rsqrt(jnp.mean(mixed * mixed, -1, keepdims=True) + HEAD_EPS)
                    * head_gain[...]
                )
                gated[rows, lanes] = (normed * (outgate / (1.0 + jnp.exp(-outgate)))).astype(BF16)
            state[...] = state[...] * ahead[block - 1 : block, :] + dot(
                value_rows, (key_rows * behind).astype(BF16), TN
            )
            return carry

        lax.fori_loop(0, ranks, at_tile, 0, unroll=True)

    def pull(start, stop):
        for item in range(start, stop):
            relay(item)
            if item + AHEAD < items:
                send_own(item + AHEAD)

    def landed(w):
        for item in range(w * cuts, (w + 1) * cuts):
            arrive(item)

    own_at = pl.ds(position(chip, core), block)

    def opening():
        for item in range(min(AHEAD, items)):
            send_own(item)
        for part in range(PARTS):
            gather_start(0, part, stream)
        rows_all[0, own_at, :] = stream[...]
        for w in range(len(locals_)):
            keep_own(w)
        pull(0, cuts)
        gathered(0, lambda rows: None)
        pull(cuts, 2 * cuts)
        landed(0)
        by_rows(gate_rows)
        pull(2 * cuts, 3 * cuts)
        landed(1)
        by_rows(up_rows)
        pull(3 * cuts, 3 * cuts + cuts // 2)
        landed(2)
        reduce_start(0, hidden, down_all)
        pull(3 * cuts + cuts // 2, 4 * cuts)
        norm_to_rows(0, norm_gain[0:1, :], BRANCH_SCALE)
        pull(4 * cuts, 5 * cuts)

    def opening_host():
        for item in range(min(HOST_AHEAD, relayed)):
            own_to(item, far_host).start()
        for part in range(PARTS):
            gather_start(0, part, stream)
        for item in range(relayed, items):
            own_to(item, near).start()
        for item in range(relayed):
            own_to(item, near).start()
        rows_all[0, own_at, :] = stream[...]
        for w in range(len(locals_)):
            keep_own(w)
        far_end = shards - 1 - near
        gates, ups, downs = (range(w * cuts, (w + 1) * cuts) for w in range(3))
        for item in gates:
            pass_on(item)
        for item in gates:
            pass_across(item, far_host)
            pass_across(item, far_end)
        for item in gates:
            send_late(item)
        for part in range(PARTS):
            guest_copy(part).wait_recv()
            gather_start(guest, part, None)
        for item in ups:
            pass_on(item)
        for owner in (far_host, far_end):
            pass_across(cuts, owner)
        gathered(0, lambda rows: None)
        for item in downs:
            pass_on(item)
        for item in ups[1:]:
            pass_across(item, far_host)
            pass_across(item, far_end)
        for item in range(relayed, items):
            own_to(item, far_host).start()
        for item in ups:
            onto(item, far_host, near).start()
        gathered(guest, lambda rows: None)
        landed(0)
        both(gate_rows)
        for item in downs:
            pass_across(item, far_host)
        pass_across(2 * cuts, far_end)
        landed(1)
        both(up_rows)
        for item in downs[1:]:
            pass_across(item, far_end)
        reduce_blocks([shard])
        down_items = range(2 * cuts, 3 * cuts)
        qkvg_items = range(3 * cuts, 4 * cuts)
        out_items = range(4 * cuts, 5 * cuts)
        for item in down_items:
            arrive_from(item, near)
        reduce_blocks([near])
        for item in qkvg_items:
            relay_from(item, far_host, near)
        relay_from(3 * cuts, near, far_host)
        for item in down_items:
            arrive_from(item, far_host)
            arrive_from(item, far_end)
        reduce_blocks([far_host, far_end])
        for item in qkvg_items[1:]:
            relay_from(item, near, far_host)
        for j in (shard, near, far_host, far_end):
            block_cross(0, j)
        relay_from(3 * cuts, far_end, near)
        reduce_own(guest)
        reduce_own(0)
        blocks_landed(guest)
        for part in range(PARTS):
            finish_norm(guest, part, norm_gain[0:1, :], BRANCH_SCALE, guest_first, 0, True)
            home_copy(part).start()
        for item in qkvg_items[1:]:
            relay_from(item, far_end, near)
        for item in out_items:
            relay_from(item, near, far_host)
            relay_from(item, far_host, near)
        blocks_landed(0)
        norm_to_rows(0, norm_gain[0:1, :], BRANCH_SCALE, True)
        for item in out_items:
            relay_from(item, far_end, near)
        for item in ups:
            onto(item, far_end, near).start()
        for item in downs:
            send_late(item)

    def opening_end():
        for item in range(cuts):
            own_to(item, home).start()
        for part in range(PARTS):
            guest_copy(part).start()
        for item in range(cuts, relayed):
            own_to(item, home).start()
        for item in direct:
            for copy in own_rest(item):
                copy.start()
        for item in range(relayed, items):
            own_to(item, home).start()
        for w in range(len(locals_)):
            keep_own(w)
        for item in range(relayed, items):
            relay(item, 1, 1)
        for item in range(relayed):
            relay(item, 1, 1)
        for item in range(cuts):
            relay(item, 2)
        for item in range(cuts, 2 * cuts):
            relay(item, 2, 2)
        for item in range(relayed, 4 * cuts):
            relay(item, 2, 2)
        relay(3 * cuts, 3)
        for part in range(PARTS):
            home_copy(part).wait_recv()
            gather_start(1, part, None)
        for item in range(3 * cuts + 1, 4 * cuts):
            relay(item, 3)

    def late(start, stop, nearest=2):
        if hosted:

            @pl.when(at_end)
            def _():
                for item in range(start, stop):
                    relay(item, nearest)

    def late_landed(w):
        if hosted:

            @pl.when(at_end)
            def _():
                landed(w)

    if hosted:
        pl.when(at_host)(opening_host)
        pl.when(at_end)(opening_end)
    else:
        opening()
    if hosted:
        for item in range(3 * cuts, 4 * cuts):
            for step in range(1, shards):
                owner = lax.rem(furthest + step, shards)

                @pl.when(owner != shard)
                def _():
                    arrive_from(item, owner)

        gathered(1, project_most)
        for item in range(3 * cuts, 4 * cuts):
            arrive_from(item, furthest)
        by_rows(project_last)
    else:
        landed(3)
        gathered(1, project_rows)
    late(4 * cuts, items)
    mix()
    late(cuts, 2 * cuts, 3)
    landed(4)
    reduce_start(1, gated, out_all)
    late(2 * cuts, 2 * cuts + 1)
    norm_to_rows(1, norm_gain[1:2, :], 1.0)
    late(2 * cuts + 1, 3 * cuts)
    late_landed(0)
    late_landed(1)
    gathered(2, hidden_rows)
    late_landed(2)
    reduce_start(2, hidden, down_all)
    for item in range(items):
        drain(item)

    def drain_rows(k, source=None):
        for part in range(PARTS):
            for copy in gather_own(k, part, source):
                copy.wait_send()
            for step in range(1, chips):
                if cores > 1:
                    forward(k, step, part).wait_send()

    def drain_sums(k):
        for part in range(PARTS):
            for step in range(1, chips):
                cross_copy(k, step, part).wait_send()
        if cores > 1:
            for chip_at in range(chips):
                part_copy(k, chip_at).wait_send()

    def drain_host():
        drain_rows(guest)
        drain_blocks(guest)
        for part in range(PARTS):
            home_copy(part).wait_send()

    def drain_end():
        for part in range(PARTS):
            guest_copy(part).wait_send()

    def drain_opening():
        drain_rows(0, stream)
        if hosted:
            drain_blocks(0)
        else:
            drain_sums(0)

    if hosted:

        @pl.when(at_host)
        def _():
            drain_opening()
            drain_host()

        pl.when(at_end)(drain_end)
    else:
        drain_opening()
    drain_rows(1)
    drain_sums(1)
    drain_rows(2)
    for part in range(PARTS):
        finish_norm(2, part, norm_gain[2:3, :], BRANCH_SCALE, result, 0)
    drain_sums(2)


def solution(mesh):
    reps, shards, ranks = mesh.shape["rep"], mesh.shape["fs"], mesh.shape["tp"]
    cores = 2 if ranks % 2 == 0 else 1
    chips = ranks // cores

    def on_device(
        stream,
        gate_weight,
        up_weight,
        down_weight,
        query_weight,
        key_weight,
        value_weight,
        outgate_weight,
        decay_down,
        decay_up,
        decay_bias,
        head_gain,
        out_weight,
        norm_gain,
    ):
        projections = (query_weight, key_weight, value_weight, outgate_weight)
        qkvg = jax.ShapeDtypeStruct((query_weight.shape[0], sum(w.shape[1] for w in projections)), BF16)
        block, width = stream.shape
        length, half_rows = block * ranks, block * chips
        hidden_width = gate_weight.shape[1]
        keys = decay_up.shape[1]
        vals = value_weight.shape[1]
        sums, pairs, levels = level_tables(block)
        vmem = pl.BlockSpec(memory_space=pltpu.VMEM)
        away = max(chips - 1, 1)
        hosted = shards == HOSTED and cores > 1 and chips > 1
        phases, slots = (4, 2) if hosted else (3, 1)
        weights = (gate_weight.T, up_weight.T, down_weight, qkvg, out_weight)
        dma = pltpu.SemaphoreType.DMA
        cuts = max(c for c in (1, CUTS) if all(w.shape[0] % (16 * reps * c) == 0 for w in weights))
        return pl.pallas_call(
            functools.partial(layer_kernel, (reps, shards, ranks, cores), levels, cuts),
            out_shape=jax.ShapeDtypeStruct((block, width), BF16),
            in_specs=[vmem] * 16,
            out_specs=vmem,
            scratch_shapes=[
                *[pltpu.VMEM((w.shape[0], shards * w.shape[1]), BF16) for w in weights[:2]],
                *[pltpu.VMEM((shards * w.shape[0], w.shape[1]), BF16) for w in weights[2:]],
                pltpu.VMEM((phases, length, width), BF16),
                pltpu.VMEM((phases, half_rows, width), BF16),
                pltpu.VMEM((phases, half_rows, width), BF16),
                pltpu.VMEM((phases, away, block, width), BF16),
                pltpu.VMEM((phases, away, block, width), BF16),
                pltpu.VMEM((slots, half_rows, width), F32),
                pltpu.VMEM((slots * length, hidden_width), F32),
                pltpu.VMEM((slots * length, hidden_width), BF16),
                pltpu.VMEM((length, qkvg.shape[1]), BF16),
                pltpu.VMEM((length, keys), F32),
                pltpu.VMEM((length, vals), BF16),
                pltpu.VMEM((vals, keys), F32),
                pltpu.VMEM((block, width), BF16),
                pltpu.VMEM(qkvg.shape, BF16),
                pltpu.VMEM((length, qkvg.shape[1]), F32),
                dma((5 * cuts, shards, reps + 1)),
                dma((5 * cuts, shards, reps)),
                dma((phases, chips, PARTS)),
                dma((phases, ranks, PARTS)),
                dma((phases, chips, PARTS)),
                dma((phases, chips, shards)),
                dma((phases, chips, shards)),
                dma((phases, away, max(PARTS, shards))),
                dma((phases, away, max(PARTS, shards))),
                *[dma((PARTS,))] * 4,
            ],
            compiler_params=pltpu.CompilerParams(
                collective_id=0, has_side_effects=True, vmem_limit_bytes=60 * 2**20
            ),
            name="layer",
        )(
            stream,
            *weights[:3],
            *projections,
            out_weight,
            decay_down.T,
            decay_up,
            decay_bias[None, :],
            head_gain[None, :],
            norm_gain,
            jnp.asarray(sums, BF16),
            jnp.asarray(pairs, F32),
        )

    in_specs = (
        P(("rep", "fs", "tp"), None),
        P("fs", "tp"),
        P("fs", "tp"),
        P("tp", "fs"),
        P("fs", "tp"),
        P("fs", "tp"),
        P("fs", "tp"),
        P("fs", "tp"),
        P(),
        P(None, "tp"),
        P("tp"),
        P(),
        P("tp", "fs"),
        P(),
    )
    return jax.shard_map(
        on_device,
        mesh=mesh,
        in_specs=in_specs,
        out_specs=P(("rep", "fs", "tp"), None),
        check_vma=False,
    )
```

```python
import functools

import jax
import jax.numpy as jnp
import numpy as np
from jax import lax
from jax.experimental import pallas as pl
from jax.experimental.pallas import tpu as pltpu
from jax.sharding import PartitionSpec as P

DK = 64
DV = 128
RESIDUAL_SCALE = 2.0**0.5
BRANCH_SCALE = 0.5
NORM_EPS = 1e-05
HEAD_EPS = 0.01
GATE_DIVISOR = 16.0
MESH = pl.DeviceIdType.MESH
CUTS = 2
AHEAD = 2
HOST_AHEAD = 2
PARTS = 4
HOSTED = 4
F32 = jnp.float32
BF16 = jnp.bfloat16
NT = (((1,), (1,)), ((), ()))
TN = (((0,), (0,)), ((), ()))


def level_tables(tile):
    row, col = np.arange(tile)[:, None], np.arange(tile)[None, :]
    sums, pairs = [], []
    half = 1
    while half < tile:
        start = row // half * half
        later = row // half % 2 == 1
        sums.append(
            np.where(later, (col >= start) & (col <= row), (col > row) & (col < start + half))
        )
        pairs.append(later & (col // half == row // half - 1))
        half *= 2
    sums += [col <= row, col > row]
    pairs.append(row == col)
    return (
        np.concatenate(sums, 0).astype(np.float32),
        np.concatenate(pairs, 0).astype(np.float32),
        len(pairs) - 1,
    )


def dot(a, b, dims=None):
    if dims is None:
        return jnp.dot(a, b, preferred_element_type=F32)
    return lax.dot_general(a, b, dims, preferred_element_type=F32)


def layer_kernel(
    sizes,
    levels,
    cuts,
    stream,
    gate_w,
    up_w,
    down_w,
    query_w,
    key_w,
    value_w,
    outgate_w,
    out_w,
    decay_down,
    decay_up,
    decay_bias,
    head_gain,
    norm_gain,
    span_sums,
    pair_masks,
    result,
    gate_all,
    up_all,
    down_all,
    qkvg_all,
    out_all,
    rows_all,
    part_out,
    part_in,
    cross_out,
    cross_in,
    partial,
    gate_buf,
    hidden,
    proj,
    log_gate,
    gated,
    state,
    guest_first,
    qkvg_w,
    proj_sums,
    decays,
    factors,
    w_send,
    w_recv,
    ag_send,
    ag_recv,
    fwd_send,
    rs_send,
    rs_recv,
    cross_send,
    cross_recv,
    guest_send,
    guest_recv,
    home_send,
    home_recv,
):
    reps, shards, ranks, cores = sizes
    chips = ranks // cores
    rep, shard, rank = lax.axis_index("rep"), lax.axis_index("fs"), lax.axis_index("tp")
    chip, core = rank // cores, lax.rem(rank, cores)
    block, width = stream.shape
    length = block * ranks
    half_rows = chips * block
    partner = {"tp": chip * cores + (cores - 1 - core)}

    barrier = pltpu.get_barrier_semaphore()

    def greet(device):
        pl.semaphore_signal(barrier, inc=1, device_id=device, device_id_type=MESH)

    @pl.when(shard > 0)
    def _():
        greet({"fs": shard - 1})

    @pl.when(shard < shards - 1)
    def _():
        greet({"fs": shard + 1})

    for step in range(1, reps):
        greet({"rep": lax.rem(rep + step, reps)})
    for step in range(1, ranks):
        greet({"tp": lax.rem(rank + step, ranks)})
    neighbours = (
        jnp.where(shard > 0, 1, 0) + jnp.where(shard < shards - 1, 1, 0) + reps - 1 + ranks - 1
    )
    pl.semaphore_wait(barrier, neighbours)

    lane = 0
    for w in (query_w, key_w, value_w, outgate_w):
        qkvg_w[:, lane : lane + w.shape[1]] = w[...]
        lane += w.shape[1]

    locals_ = (gate_w, up_w, down_w, qkvg_w, out_w)
    hosted = shards == HOSTED and cores > 1 and chips > 1
    guest = 3
    relayed = 3 * cuts
    items = len(locals_) * cuts
    direct = range(cuts // 2, 3 * cuts)
    at_end = (shard == 0) | (shard == shards - 1)
    at_host = jnp.logical_not(at_end)
    near = jnp.where(shard < shards // 2, 0, shards - 1)
    home = jnp.where(shard < shards // 2, 1, shards - 2)
    far_host = shards - 1 - shard

    def is_host(at):
        return (at > 0) & (at < shards - 1)

    wholes = (gate_all, up_all, down_all, qkvg_all, out_all)

    def side_by_side(w):
        return wholes[w].shape[0] == locals_[w].shape[0]

    def piece(item, owner, part):
        w, cut = item // cuts, item % cuts
        rows, columns = locals_[w].shape
        size = rows // (reps * cuts)
        start = (part * cuts + cut) * size
        if side_by_side(w):
            return wholes[w].at[
                pl.ds(pl.multiple_of(start, size), size),
                pl.ds(pl.multiple_of(owner * columns, columns), columns),
            ]
        return wholes[w].at[pl.ds(pl.multiple_of(owner * rows + start, size), size), :]

    def own_piece(item, part=rep):
        w, cut = item // cuts, item % cuts
        size = locals_[w].shape[0] // (reps * cuts)
        return locals_[w].at[pl.ds(pl.multiple_of((part * cuts + cut) * size, size), size), :]

    def weight_copy(w, owner, part, slot, device, source=None):
        target = piece(w, owner, part)
        return pltpu.make_async_remote_copy(
            src_ref=target if source is None else source,
            dst_ref=target,
            send_sem=w_send.at[w, owner, slot],
            recv_sem=w_recv.at[w, owner, part],
            device_id=device,
            device_id_type=MESH,
        )

    def own_right(w):
        return weight_copy(w, shard, rep, 0, {"fs": shard + 1}, own_piece(w))

    def own_left(w):
        return weight_copy(w, shard, rep, reps, {"fs": shard - 1}, own_piece(w))

    def send_own(w):
        @pl.when(shard < shards - 1)
        def _():
            own_right(w).start()

        @pl.when(shard > 0)
        def _():
            own_left(w).start()

    def own_to(item, toward):
        slot = jnp.where(toward > shard, 0, reps)
        return weight_copy(item, shard, rep, slot, {"fs": toward}, own_piece(item))

    def own_rest(item):
        copies = []
        for step in range(1, reps):
            part = lax.rem(rep + step, reps)
            source = own_piece(item, part)
            copies.append(weight_copy(item, shard, part, step, {"fs": home}, source))
        return copies

    def keep_own(w):
        rows, columns = locals_[w].shape
        if side_by_side(w):
            at = pl.ds(pl.multiple_of(shard * columns, columns), columns)
            wholes[w][:, at] = locals_[w][...]
        else:
            wholes[w][pl.ds(pl.multiple_of(shard * rows, rows), rows), :] = locals_[w][...]

    def others(body, nearest=1, furthest=shards - 1):
        def at_distance(d, carry):
            for sign in (-1, 1):
                owner = shard + sign * d

                @pl.when((owner >= 0) & (owner < shards))
                def _():
                    body(owner, shard - sign)

            return carry

        lax.fori_loop(nearest, furthest + 1, at_distance, 0)

    def onto(item, owner, onward):
        return weight_copy(item, owner, rep, 0, {"fs": onward})

    def sideways(item, owner):
        return [
            weight_copy(item, owner, rep, step, {"rep": lax.rem(rep + step, reps)})
            for step in range(1, reps)
        ]

    def relay(item, nearest=1, furthest=shards - 1):
        def body(owner, onward):
            weight_copy(item, owner, rep, 0, partner).wait_recv()

            @pl.when((onward >= 0) & (onward < shards))
            def _():
                onto(item, owner, onward).start()

            for copy in sideways(item, owner):
                copy.start()

        others(body, nearest, furthest)

    def relay_from(item, owner, onward):
        weight_copy(item, owner, rep, 0, partner).wait_recv()
        onto(item, owner, onward).start()
        for copy in sideways(item, owner):
            copy.start()

    def pass_on(item):
        weight_copy(item, near, rep, 0, partner).wait_recv()
        onto(item, near, far_host).start()
        if item not in direct:
            for copy in sideways(item, near):
                copy.start()
        if item + HOST_AHEAD < relayed:
            own_to(item + HOST_AHEAD, far_host).start()

    def pass_across(item, owner):
        weight_copy(item, owner, rep, 0, partner).wait_recv()
        for copy in sideways(item, owner):
            copy.start()

    def send_late(item):
        def body(owner, onward):
            @pl.when(jnp.logical_not(is_host(onward)))
            def _():
                onto(item, owner, onward).start()

        others(body)

    def arrive(w):
        def body(owner, onward):
            for step in range(1, reps):
                weight_copy(w, owner, lax.rem(rep + step, reps), step, partner).wait_recv()

        others(body)

    def arrive_from(item, owner):
        for step in range(1, reps):
            weight_copy(item, owner, lax.rem(rep + step, reps), step, partner).wait_recv()

    def drain(item):
        @pl.when(shard < shards - 1)
        def _():
            own_right(item).wait_send()

        @pl.when(shard > 0)
        def _():
            own_left(item).wait_send()

        first = hosted and item in direct
        if first:

            @pl.when(at_end)
            def _():
                for copy in own_rest(item):
                    copy.wait_send()

        def body(owner, onward):
            @pl.when((onward >= 0) & (onward < shards))
            def _():
                onto(item, owner, onward).wait_send()

            @pl.when(jnp.logical_not(first & at_host & is_host(onward)))
            def _():
                for copy in sideways(item, owner):
                    copy.wait_send()

        others(body)

    def position(chip_at, core_at):
        return pl.multiple_of((core_at * chips + chip_at) * block, block)

    strip = block // PARTS

    fold = 2 if hosted else 1
    lap = block // fold

    def row_at(k, chip_at, core_at, offset):
        if k != 2:
            return position(chip_at, core_at) + offset
        return (chip_at * fold + offset // lap) * cores * lap + core_at * lap + offset % lap

    def row_copy(k, chip_at, core_at, send, part, device, source=None):
        at = pl.multiple_of(row_at(k, chip_at, core_at, part * strip), strip)
        target = rows_all.at[k, pl.ds(at, strip), :]
        return pltpu.make_async_remote_copy(
            src_ref=target if source is None else source.at[pl.ds(part * strip, strip), :],
            dst_ref=target,
            send_sem=send.at[part],
            recv_sem=ag_recv.at[k, core_at * chips + chip_at, part],
            device_id=device,
            device_id_type=MESH,
        )

    def guest_copy(part):
        at = pl.multiple_of(position(chip, core) + part * strip, strip)
        return pltpu.make_async_remote_copy(
            src_ref=stream.at[pl.ds(part * strip, strip), :],
            dst_ref=rows_all.at[guest, pl.ds(at, strip), :],
            send_sem=guest_send.at[part],
            recv_sem=guest_recv.at[part],
            device_id={"fs": home},
            device_id_type=MESH,
        )

    def home_copy(part):
        at = pl.multiple_of(position(chip, core) + part * strip, strip)
        return pltpu.make_async_remote_copy(
            src_ref=guest_first.at[pl.ds(part * strip, strip), :],
            dst_ref=rows_all.at[1, pl.ds(at, strip), :],
            send_sem=home_send.at[part],
            recv_sem=home_recv.at[part],
            device_id={"fs": near},
            device_id_type=MESH,
        )

    def chip_away(step):
        return lax.rem(chip + step, chips)

    def gather_own(k, part, source):
        copies = []
        for step in range(1, chips):
            device = {"tp": chip_away(step) * cores + core}
            copies.append(row_copy(k, chip, core, ag_send.at[k, step], part, device, source))
        if cores > 1:
            copies.append(row_copy(k, chip, core, ag_send.at[k, 0], part, partner, source))
        return copies

    def forward(k, step, part):
        return row_copy(k, chip_away(step), core, fwd_send.at[k, step], part, partner)

    def mirrored(k, step, part):
        return row_copy(
            k, chip_away(step), cores - 1 - core, fwd_send.at[k, step], part, partner
        )

    def gather_start(k, part, source):
        for copy in gather_own(k, part, source):
            copy.start()

    def gathered(k, body):
        if cores > 1:
            for part in range(PARTS):
                mirrored(k, 0, part).wait_recv()

        def at_core(n, carry):
            body(pl.ds(pl.multiple_of(row_at(k, chip, n, 0), block), block))
            return carry

        lax.fori_loop(0, cores, at_core, 0)
        for step in range(1, chips):
            for part in range(PARTS):
                forward(k, step, part).wait_recv()
                if cores > 1:
                    forward(k, step, part).start()

            def at_turn(n, carry):
                @pl.when(n == 1)
                def _():
                    for part in range(PARTS):
                        mirrored(k, step, part).wait_recv()

                turn = jnp.where(n == 0, core, cores - 1 - core)
                body(pl.ds(pl.multiple_of(row_at(k, chip_away(step), turn, 0), block), block))
                return carry

            lax.fori_loop(0, cores, at_turn, 0)

    def part_copy(k, chip_at):
        rows = pl.ds(pl.multiple_of(chip_at * block, block), block)
        return pltpu.make_async_remote_copy(
            src_ref=part_out.at[k, rows, :],
            dst_ref=part_in.at[k, rows, :],
            send_sem=rs_send.at[k, chip_at, 0],
            recv_sem=rs_recv.at[k, lax.rem(chip_at - chip + chips, chips), 0],
            device_id=partner,
            device_id_type=MESH,
        )

    def cross_copy(k, step, part):
        rows = pl.ds(part * strip, strip)
        return pltpu.make_async_remote_copy(
            src_ref=cross_out.at[k, step - 1, rows, :],
            dst_ref=cross_in.at[k, step - 1, rows, :],
            send_sem=cross_send.at[k, step - 1, part],
            recv_sem=cross_recv.at[k, step - 1, part],
            device_id={"tp": chip_away(step) * cores + core},
            device_id_type=MESH,
        )

    def product(k, left, weights, core_at, chip_at, into):
        depth, columns = weights.shape[0] // shards, weights.shape[1]
        at = row_at(k, chip_at, core_at, 0)
        rows = left[pl.ds(pl.multiple_of(at, block), block), :]
        to = pl.ds(pl.multiple_of(chip_at * block, block), block)

        def at_shard(j, carry):
            value = dot(rows, weights[pl.ds(pl.multiple_of(j * depth, depth), depth), :])
            into[to, pl.ds(pl.multiple_of(j * columns, columns), columns)] = value.astype(
                into.dtype
            )
            return carry

        lax.fori_loop(0, shards, at_shard, 0)

    def reduce_start(k, left, weights):
        sums = partial.at[k // 3]

        for step in range(1, chips + 1):
            away = chip_away(step)
            if cores > 1:
                product(k, left, weights, cores - 1 - core, away, part_out.at[k])
                part_copy(k, away).start()
            product(k, left, weights, core, away, sums)
            if step < chips:
                if cores > 1:
                    part_copy(k, away).wait_recv()
                for part in range(PARTS):
                    rows = pl.ds(pl.multiple_of(away * block + part * strip, strip), strip)
                    value = sums[rows, :]
                    if cores > 1:
                        value = value + part_in[k, rows, :].astype(F32)
                    cross_out[k, step - 1, part * strip : (part + 1) * strip, :] = value.astype(
                        BF16
                    )
                    cross_copy(k, step, part).start()
        if cores > 1:
            part_copy(k, chip).wait_recv()

    depth, columns = locals_[2].shape

    def block_at(chip_at, j):
        return (
            pl.ds(pl.multiple_of(chip_at * block, block), block),
            pl.ds(pl.multiple_of(j * columns, columns), columns),
        )

    def part_block(k, chip_at, j):
        at = block_at(chip_at, j)
        return pltpu.make_async_remote_copy(
            src_ref=part_out.at[k, at[0], at[1]],
            dst_ref=part_in.at[k, at[0], at[1]],
            send_sem=rs_send.at[k, chip_at, j],
            recv_sem=rs_recv.at[k, lax.rem(chip_at - chip + chips, chips), j],
            device_id=partner,
            device_id_type=MESH,
        )

    def cross_block(k, step, j):
        at = block_at(0, j)[1]
        return pltpu.make_async_remote_copy(
            src_ref=cross_out.at[k, step - 1, :, at],
            dst_ref=cross_in.at[k, step - 1, :, at],
            send_sem=cross_send.at[k, step - 1, j],
            recv_sem=cross_recv.at[k, step - 1, j],
            device_id={"tp": chip_away(step) * cores + core},
            device_id_type=MESH,
        )

    def block_product(k, core_at, chip_at, j):
        rows = pl.ds(pl.multiple_of(k // 3 * length + position(chip_at, core_at), block), block)
        return dot(hidden[rows, :], down_all[pl.ds(pl.multiple_of(j * depth, depth), depth), :])

    def block_parts(k, chip_at, j):
        rows, at = block_at(chip_at, j)
        part_out[k, rows, at] = block_product(k, cores - 1 - core, chip_at, j).astype(BF16)
        part_block(k, chip_at, j).start()
        partial[k // 3, rows, at] = block_product(k, core, chip_at, j)

    def block_cross(k, j):
        for step in range(1, chips):
            away = chip_away(step)
            rows, at = block_at(away, j)
            part_block(k, away, j).wait_recv()
            value = partial[k // 3, rows, at] + part_in[k, rows, at].astype(F32)
            cross_out[k, step - 1, :, at] = value.astype(BF16)
            cross_block(k, step, j).start()

    def reduce_blocks(owners, early=False):
        for k in (guest, 0):
            for j in owners:
                for step in range(1, chips):
                    block_parts(k, chip_away(step), j)
            if k == guest or early:
                for j in owners:
                    block_cross(k, j)

    def reduce_own(k):
        def at_shard(j, carry):
            block_parts(k, chip, j)
            return carry

        lax.fori_loop(0, shards, at_shard, 0)

    def blocks_landed(k):
        def at_shard(j, carry):
            part_block(k, chip, j).wait_recv()
            for step in range(1, chips):
                cross_block(k, step, j).wait_recv()
            return carry

        lax.fori_loop(0, shards, at_shard, 0)

    def drain_blocks(k):
        def at_shard(j, carry):
            for chip_at in range(chips):
                part_block(k, chip_at, j).wait_send()
            for step in range(1, chips):
                cross_block(k, step, j).wait_send()
            return carry

        lax.fori_loop(0, shards, at_shard, 0)

    def part_lap(chip_at, h):
        rows = pl.ds(pl.multiple_of(chip_at * block + h * lap, lap), lap)
        return pltpu.make_async_remote_copy(
            src_ref=part_out.at[2, rows, :],
            dst_ref=part_in.at[2, rows, :],
            send_sem=rs_send.at[2, chip_at, h],
            recv_sem=rs_recv.at[2, lax.rem(chip_at - chip + chips, chips), h],
            device_id=partner,
            device_id_type=MESH,
        )

    def lap_product(core_at, chip_at, h, into):
        left = pl.ds(pl.multiple_of(row_at(2, chip_at, core_at, h * lap), lap), lap)
        to = pl.ds(pl.multiple_of(chip_at * block + h * lap, lap), lap)

        def at_shard(j, carry):
            value = dot(hidden[left, :], down_all[pl.ds(pl.multiple_of(j * depth, depth), depth), :])
            into[to, pl.ds(pl.multiple_of(j * columns, columns), columns)] = value.astype(into.dtype)
            return carry

        lax.fori_loop(0, shards, at_shard, 0)

    def lap_parts(chip_at, h):
        lap_product(cores - 1 - core, chip_at, h, part_out.at[2])
        part_lap(chip_at, h).start()
        lap_product(core, chip_at, h, partial.at[0])

    def second_block():
        per_lap = PARTS // fold
        for part in range(PARTS):
            mirrored(2, 0, part).wait_recv()
        hidden_rows(pl.ds(pl.multiple_of(chip * cores * block, cores * block), cores * block))
        for h in range(fold):
            parts = range(h * per_lap, (h + 1) * per_lap)
            for step in range(1, chips):
                for part in parts:
                    forward(2, step, part).wait_recv()
                    forward(2, step, part).start()
            for step in range(1, chips):
                away = chip_away(step)
                for part in parts:
                    mirrored(2, step, part).wait_recv()
                at = (away * fold + h) * cores * lap
                hidden_rows(pl.ds(pl.multiple_of(at, cores * lap), cores * lap))
                if h == 0:
                    late_landed(2)
                lap_parts(away, h)
                part_lap(away, h).wait_recv()
                for part in parts:
                    rows = pl.ds(pl.multiple_of(away * block + part * strip, strip), strip)
                    value = partial[0, rows, :] + part_in[2, rows, :].astype(F32)
                    cross_out[2, step - 1, part * strip : (part + 1) * strip, :] = value.astype(BF16)
                    cross_copy(2, step, part).start()
        for h in range(fold):
            lap_parts(chip, h)
        for h in range(fold):
            part_lap(chip, h).wait_recv()

    def drain_laps():
        for h in range(fold):
            for chip_at in range(chips):
                part_lap(chip_at, h).wait_send()
        for part in range(PARTS):
            for step in range(1, chips):
                cross_copy(2, step, part).wait_send()

    chunk = min(32, strip)

    def finish_norm(k, part, scale, branch, into, into_at, blocks=False):
        if not blocks:
            for step in range(1, chips):
                cross_copy(k, step, part).wait_recv()

        def at_chunk(n, carry):
            rows = pl.ds(pl.multiple_of(chip * block + n * chunk, chunk), chunk)
            inner = pl.ds(pl.multiple_of(n * chunk, chunk), chunk)
            summed = partial[k // 3, rows, :]
            if cores > 1:
                summed = summed + part_in[k, rows, :].astype(F32)
            for step in range(1, chips):
                summed = summed + cross_in[k, step - 1, inner, :].astype(F32)
            current = rows_all[
                k, pl.ds(pl.multiple_of(row_at(k, chip, core, n * chunk), chunk), chunk), :
            ].astype(F32)
            values = RESIDUAL_SCALE * current + (summed if branch == 1.0 else branch * summed)
            centred = values - jnp.mean(values, -1, keepdims=True)
            spread = jnp.mean(centred * centred, -1, keepdims=True)
            done = (centred * lax.rsqrt(spread + NORM_EPS) * scale).astype(BF16)
            into[pl.ds(pl.multiple_of(into_at(n * chunk), chunk), chunk), :] = done
            return carry

        lax.fori_loop(part * strip // chunk, (part + 1) * strip // chunk, at_chunk, 0)

    def norm_to_rows(k, scale, branch, blocks=False, meanwhile=None):
        for part in range(PARTS):
            if meanwhile is not None and part == 1:
                meanwhile()
            finish_norm(
                k, part, scale, branch, rows_all.at[k + 1],
                lambda offset: row_at(k + 1, chip, core, offset), blocks,
            )
            gather_start(k + 1, part, None)

    high = min(256, length)

    def by_rows(body):
        def at_rows(m, carry):
            body(pl.ds(pl.multiple_of(m * high, high), high))
            return carry

        lax.fori_loop(0, length // high, at_rows, 0)

    def silu(values):
        return values / (1.0 + jnp.exp(-values))

    def shifted(rows, slot):
        return pl.ds(pl.multiple_of(rows.start + slot * length, high), high)

    def gate_rows(rows, k=0, slot=0):
        gate_buf[shifted(rows, slot), :] = silu(dot(rows_all[k, rows, :], gate_all[...], NT))

    def up_rows(rows, k=0, slot=0):
        upward = dot(rows_all[k, rows, :], up_all[...], NT)
        at = shifted(rows, slot)
        hidden[at, :] = (gate_buf[at, :] * upward).astype(BF16)

    def both(rows_body):
        by_rows(rows_body)
        by_rows(lambda rows: rows_body(rows, guest, 1))

    def hidden_rows(rows):
        upward = dot(rows_all[2, rows, :], up_all[...], NT)
        gate = silu(dot(rows_all[2, rows, :], gate_all[...], NT))
        hidden[rows, :] = (gate * upward).astype(BF16)

    keys = decay_up.shape[1]
    heads = keys // DK
    vals = heads * DV

    furthest = jnp.where(at_end, shards - 1 - shard, shards - 1 - near)

    def slab(rows, j):
        deep = qkvg_w.shape[0]
        at = pl.ds(pl.multiple_of(j * deep, deep), deep)
        return dot(rows_all[1, rows, at], qkvg_all[at, :])

    def project_most(rows):
        decay_rows(rows)
        total = slab(rows, lax.rem(furthest + 1, shards))
        for step in range(2, shards):
            total = total + slab(rows, lax.rem(furthest + step, shards))
        proj_sums[rows, :] = total

    def project_last(rows):
        proj[rows, :] = (proj_sums[rows, :] + slab(rows, furthest)).astype(BF16)

    def project_rows(rows):
        decay_rows(rows)
        proj[rows, :] = dot(rows_all[1, rows, :], qkvg_all[...]).astype(BF16)

    def decay_rows(rows):
        low = dot(rows_all[1, rows, :], decay_down[...], NT).astype(BF16)
        pre = dot(low, decay_up[...]) + decay_bias[...]
        log_gate[rows, :] = (
            jnp.minimum(pre, 0.0) - jnp.log1p(jnp.exp(-jnp.abs(pre)))
        ) / GATE_DIVISOR

    bulk = keys % 128 == 0

    def spread():
        for n in range(ranks):
            rows = pl.ds(position(n // cores, n % cores), block)
            decay = log_gate[rows, :]
            coarse = decay.astype(BF16)
            lanes = slice(n * keys, (n + 1) * keys)
            decays[0:block, lanes] = coarse
            decays[block : 2 * block, lanes] = (decay - coarse.astype(F32)).astype(BF16)

        def at_table(at, carry):
            rows = pl.ds(pl.multiple_of(at * block, block), block)
            factors[rows, :] = jnp.exp(dot(span_sums[rows, :], decays[...]))
            return carry

        lax.fori_loop(0, levels + 2, at_table, 0)

    def mix():
        lane_head = lax.broadcasted_iota(jnp.int32, (1, keys), 1) // DK
        lane_masks = [jnp.where(lane_head == h, 1.0, 0.0) for h in range(heads)]
        state[...] = jnp.zeros_like(state)

        def at_tile(n, carry):
            rows = pl.ds(position(n // cores, lax.rem(n, cores)), block)
            query = proj[rows, 0:keys].astype(F32) * DK ** (-0.5)
            key_rows = proj[rows, keys : 2 * keys].astype(F32)
            value_rows = proj[rows, 2 * keys : 2 * keys + vals]
            decay = log_gate[rows, :]
            coarse = decay.astype(BF16)
            fine = (decay - coarse.astype(F32)).astype(BF16)

            def weight(at):
                if bulk:
                    lanes = pl.ds(pl.multiple_of(n * keys, keys), keys)
                    return factors[at * block : (at + 1) * block, lanes]
                table = span_sums[at * block : (at + 1) * block, 0:block]
                return jnp.exp(dot(table, coarse) + dot(table, fine))

            scores = [jnp.zeros((block, block), F32) for _ in range(heads)]
            for at in range(levels + 1):
                pairs = pair_masks[at * block : (at + 1) * block, :]
                if at < levels:
                    factor = weight(at)
                    late, early = query * factor, (key_rows * factor).astype(BF16)
                else:
                    late, early = query, key_rows.astype(BF16)
                for h in range(heads):
                    scores[h] = scores[h] + pairs * dot(
                        (late * lane_masks[h]).astype(BF16), early, NT
                    )
            ahead = weight(levels)
            behind = weight(levels + 1)
            late = query * ahead
            held = state[...].astype(BF16)
            for h in range(heads):
                lanes = slice(h * DV, (h + 1) * DV)
                mixed = dot(scores[h].astype(BF16), value_rows[:, lanes]) + dot(
                    (late * lane_masks[h]).astype(BF16), held[lanes, :], NT
                )
                outgate = proj[
                    rows, 2 * keys + vals + h * DV : 2 * keys + vals + (h + 1) * DV
                ].astype(F32)
                normed = (
                    mixed
                    * lax.rsqrt(jnp.mean(mixed * mixed, -1, keepdims=True) + HEAD_EPS)
                    * head_gain[...]
                )
                gated[rows, lanes] = (normed * (outgate / (1.0 + jnp.exp(-outgate)))).astype(BF16)
            state[...] = state[...] * ahead[block - 1 : block, :] + dot(
                value_rows, (key_rows * behind).astype(BF16), TN
            )
            return carry

        lax.fori_loop(0, ranks, at_tile, 0, unroll=True)

    def pull(start, stop):
        for item in range(start, stop):
            relay(item)
            if item + AHEAD < items:
                send_own(item + AHEAD)

    def landed(w):
        for item in range(w * cuts, (w + 1) * cuts):
            arrive(item)

    own_at = pl.ds(position(chip, core), block)

    def opening():
        for item in range(min(AHEAD, items)):
            send_own(item)
        for part in range(PARTS):
            gather_start(0, part, stream)
        rows_all[0, own_at, :] = stream[...]
        for w in range(len(locals_)):
            keep_own(w)
        pull(0, cuts)
        gathered(0, lambda rows: None)
        pull(cuts, 2 * cuts)
        landed(0)
        by_rows(gate_rows)
        pull(2 * cuts, 3 * cuts)
        landed(1)
        by_rows(up_rows)
        pull(3 * cuts, 3 * cuts + cuts // 2)
        landed(2)
        reduce_start(0, hidden, down_all)
        pull(3 * cuts + cuts // 2, 4 * cuts)
        norm_to_rows(0, norm_gain[0:1, :], BRANCH_SCALE)
        pull(4 * cuts, 5 * cuts)

    def opening_host():
        for item in range(min(HOST_AHEAD, relayed)):
            own_to(item, far_host).start()
        for part in range(PARTS):
            gather_start(0, part, stream)
        for item in range(relayed, items):
            own_to(item, near).start()
        for item in range(relayed):
            own_to(item, near).start()
        rows_all[0, own_at, :] = stream[...]
        for w in range(len(locals_)):
            keep_own(w)
        far_end = shards - 1 - near
        gates, ups, downs = (range(w * cuts, (w + 1) * cuts) for w in range(3))
        for item in gates:
            pass_on(item)
        for item in gates:
            pass_across(item, far_host)
            pass_across(item, far_end)
        for item in gates:
            send_late(item)
        for part in range(PARTS):
            guest_copy(part).wait_recv()
            gather_start(guest, part, None)
        for item in ups:
            pass_on(item)
        for owner in (far_host, far_end):
            pass_across(cuts, owner)
        gathered(0, lambda rows: None)
        for item in downs:
            pass_on(item)
        for item in ups[1:]:
            pass_across(item, far_host)
            pass_across(item, far_end)
        for item in range(relayed, items):
            own_to(item, far_host).start()
        for item in ups:
            onto(item, far_host, near).start()
        gathered(guest, lambda rows: None)
        landed(0)
        both(gate_rows)
        for item in downs:
            pass_across(item, far_host)
        pass_across(2 * cuts, far_end)
        landed(1)
        both(up_rows)
        for item in downs[1:]:
            pass_across(item, far_end)
        reduce_blocks([shard], True)
        down_items = range(2 * cuts, 3 * cuts)
        qkvg_items = range(3 * cuts, 4 * cuts)
        out_items = range(4 * cuts, 5 * cuts)
        for item in down_items:
            arrive_from(item, near)
        reduce_blocks([near])
        for item in (*qkvg_items, *out_items):
            relay_from(item, far_host, near)
        relay_from(3 * cuts, near, far_host)
        for item in down_items:
            arrive_from(item, far_host)
            arrive_from(item, far_end)
        reduce_blocks([far_host, far_end])
        for item in qkvg_items[1:]:
            relay_from(item, near, far_host)
        for j in (near, far_host, far_end):
            block_cross(0, j)
        relay_from(3 * cuts, far_end, near)
        reduce_own(guest)
        reduce_own(0)
        blocks_landed(guest)
        for part in range(PARTS):
            finish_norm(guest, part, norm_gain[0:1, :], BRANCH_SCALE, guest_first, lambda offset: offset, True)
            home_copy(part).start()
        for item in qkvg_items[1:]:
            relay_from(item, far_end, near)
        for item in out_items:
            relay_from(item, near, far_host)
        blocks_landed(0)
        norm_to_rows(0, norm_gain[0:1, :], BRANCH_SCALE, True)
        for item in out_items:
            relay_from(item, far_end, near)
        for item in ups:
            onto(item, far_end, near).start()
        for item in downs:
            send_late(item)

    def opening_end():
        for item in range(cuts):
            own_to(item, home).start()
        for part in range(PARTS):
            guest_copy(part).start()
        for item in range(cuts, relayed):
            own_to(item, home).start()
        for item in direct:
            for copy in own_rest(item):
                copy.start()
        for item in range(relayed, items):
            own_to(item, home).start()
        for w in range(len(locals_)):
            keep_own(w)
        for item in range(relayed, items):
            relay(item, 1, 1)
        for item in range(relayed):
            relay(item, 1, 1)
        for item in range(cuts):
            relay(item, 2)
        for item in range(cuts, 2 * cuts):
            relay(item, 2, 2)
        for item in range(relayed, 4 * cuts):
            relay(item, 2, 2)
        for item in range(4 * cuts, items):
            relay(item, 2, 2)
        relay(3 * cuts, 3)
        for part in range(PARTS):
            home_copy(part).wait_recv()
            gather_start(1, part, None)
        for item in range(3 * cuts + 1, 4 * cuts):
            relay(item, 3)

    def late(start, stop, nearest=2):
        if hosted:

            @pl.when(at_end)
            def _():
                for item in range(start, stop):
                    relay(item, nearest)

    def late_landed(w):
        if hosted:

            @pl.when(at_end)
            def _():
                landed(w)

    if hosted:
        pl.when(at_host)(opening_host)
        pl.when(at_end)(opening_end)
    else:
        opening()
    if hosted:
        for item in range(3 * cuts, 4 * cuts):
            for step in range(1, shards):
                owner = lax.rem(furthest + step, shards)

                @pl.when(owner != shard)
                def _():
                    arrive_from(item, owner)

        gathered(1, project_most)
        if bulk:
            spread()
        late(4 * cuts, items, 3)
        for item in range(3 * cuts, 4 * cuts):
            arrive_from(item, furthest)
        by_rows(project_last)
    else:
        landed(3)
        gathered(1, project_rows)
        if bulk:
            spread()
    mix()
    late(cuts, cuts + 1, 3)
    landed(4)
    late(cuts + 1, 2 * cuts, 3)
    reduce_start(1, gated, out_all)
    norm_to_rows(
        1, norm_gain[1:2, :], 1.0, meanwhile=lambda: late(2 * cuts, 2 * cuts + 1)
    )
    late(2 * cuts + 1, 3 * cuts)
    late_landed(0)
    late_landed(1)
    if hosted:
        second_block()
    else:
        gathered(2, hidden_rows)
        reduce_start(2, hidden, down_all)
    for item in range(items):
        drain(item)

    def drain_rows(k, source=None):
        for part in range(PARTS):
            for copy in gather_own(k, part, source):
                copy.wait_send()
            for step in range(1, chips):
                if cores > 1:
                    forward(k, step, part).wait_send()

    def drain_sums(k):
        for part in range(PARTS):
            for step in range(1, chips):
                cross_copy(k, step, part).wait_send()
        if cores > 1:
            for chip_at in range(chips):
                part_copy(k, chip_at).wait_send()

    def drain_host():
        drain_rows(guest)
        drain_blocks(guest)
        for part in range(PARTS):
            home_copy(part).wait_send()

    def drain_end():
        for part in range(PARTS):
            guest_copy(part).wait_send()

    def drain_opening():
        drain_rows(0, stream)
        if hosted:
            drain_blocks(0)
        else:
            drain_sums(0)

    if hosted:

        @pl.when(at_host)
        def _():
            drain_opening()
            drain_host()

        pl.when(at_end)(drain_end)
    else:
        drain_opening()
    drain_rows(1)
    drain_sums(1)
    drain_rows(2)
    for part in range(PARTS):
        finish_norm(2, part, norm_gain[2:3, :], BRANCH_SCALE, result, lambda offset: offset)
    if hosted:
        drain_laps()
    else:
        drain_sums(2)


def solution(mesh):
    reps, shards, ranks = mesh.shape["rep"], mesh.shape["fs"], mesh.shape["tp"]
    cores = 2 if ranks % 2 == 0 else 1
    chips = ranks // cores

    def on_device(
        stream,
        gate_weight,
        up_weight,
        down_weight,
        query_weight,
        key_weight,
        value_weight,
        outgate_weight,
        decay_down,
        decay_up,
        decay_bias,
        head_gain,
        out_weight,
        norm_gain,
    ):
        projections = (query_weight, key_weight, value_weight, outgate_weight)
        qkvg = jax.ShapeDtypeStruct((query_weight.shape[0], sum(w.shape[1] for w in projections)), BF16)
        block, width = stream.shape
        length, half_rows = block * ranks, block * chips
        hidden_width = gate_weight.shape[1]
        keys = decay_up.shape[1]
        vals = value_weight.shape[1]
        sums, pairs, levels = level_tables(block)
        vmem = pl.BlockSpec(memory_space=pltpu.VMEM)
        away = max(chips - 1, 1)
        hosted = shards == HOSTED and cores > 1 and chips > 1
        phases, slots = (4, 2) if hosted else (3, 1)
        weights = (gate_weight.T, up_weight.T, down_weight, qkvg, out_weight)
        dma = pltpu.SemaphoreType.DMA
        cuts = max(c for c in (1, CUTS) if all(w.shape[0] % (16 * reps * c) == 0 for w in weights))
        return pl.pallas_call(
            functools.partial(layer_kernel, (reps, shards, ranks, cores), levels, cuts),
            out_shape=jax.ShapeDtypeStruct((block, width), BF16),
            in_specs=[vmem] * 16,
            out_specs=vmem,
            scratch_shapes=[
                *[pltpu.VMEM((w.shape[0], shards * w.shape[1]), BF16) for w in weights[:2]],
                *[pltpu.VMEM((shards * w.shape[0], w.shape[1]), BF16) for w in weights[2:]],
                pltpu.VMEM((phases, length, width), BF16),
                pltpu.VMEM((phases, half_rows, width), BF16),
                pltpu.VMEM((phases, half_rows, width), BF16),
                pltpu.VMEM((phases, away, block, width), BF16),
                pltpu.VMEM((phases, away, block, width), BF16),
                pltpu.VMEM((slots, half_rows, width), F32),
                pltpu.VMEM((slots * length, hidden_width), F32),
                pltpu.VMEM((slots * length, hidden_width), BF16),
                pltpu.VMEM((length, qkvg.shape[1]), BF16),
                pltpu.VMEM((length, keys), F32),
                pltpu.VMEM((length, vals), BF16),
                pltpu.VMEM((vals, keys), F32),
                pltpu.VMEM((block, width), BF16),
                pltpu.VMEM(qkvg.shape, BF16),
                pltpu.VMEM((length, qkvg.shape[1]), F32),
                pltpu.VMEM((2 * block, ranks * keys), BF16),
                pltpu.VMEM(((levels + 2) * block, ranks * keys), F32),
                dma((5 * cuts, shards, reps + 1)),
                dma((5 * cuts, shards, reps)),
                dma((phases, chips, PARTS)),
                dma((phases, ranks, PARTS)),
                dma((phases, chips, PARTS)),
                dma((phases, chips, shards)),
                dma((phases, chips, shards)),
                dma((phases, away, max(PARTS, shards))),
                dma((phases, away, max(PARTS, shards))),
                *[dma((PARTS,))] * 4,
            ],
            compiler_params=pltpu.CompilerParams(
                collective_id=0, has_side_effects=True, vmem_limit_bytes=60 * 2**20
            ),
            name="layer",
        )(
            stream,
            *weights[:3],
            *projections,
            out_weight,
            decay_down.T,
            decay_up,
            decay_bias[None, :],
            head_gain[None, :],
            norm_gain,
            jnp.asarray(np.concatenate([sums, sums], 1), BF16),
            jnp.asarray(pairs, F32),
        )

    in_specs = (
        P(("rep", "fs", "tp"), None),
        P("fs", "tp"),
        P("fs", "tp"),
        P("tp", "fs"),
        P("fs", "tp"),
        P("fs", "tp"),
        P("fs", "tp"),
        P("fs", "tp"),
        P(),
        P(None, "tp"),
        P("tp"),
        P(),
        P("tp", "fs"),
        P(),
    )
    return jax.shard_map(
        on_device,
        mesh=mesh,
        in_specs=in_specs,
        out_specs=P(("rep", "fs", "tp"), None),
        check_vma=False,
    )
```

```python
import functools

import jax
import jax.numpy as jnp
import numpy as np
from jax import lax
from jax.experimental import pallas as pl
from jax.experimental.pallas import tpu as pltpu
from jax.sharding import PartitionSpec as P

DK = 64
DV = 128
RESIDUAL_SCALE = 2.0**0.5
BRANCH_SCALE = 0.5
NORM_EPS = 1e-05
HEAD_EPS = 0.01
GATE_DIVISOR = 16.0
MESH = pl.DeviceIdType.MESH
CUTS = 2
AHEAD = 2
HOST_AHEAD = 2
PARTS = 4
HOSTED = 4
F32 = jnp.float32
BF16 = jnp.bfloat16
NT = (((1,), (1,)), ((), ()))
TN = (((0,), (0,)), ((), ()))


def level_tables(tile):
    row, col = np.arange(tile)[:, None], np.arange(tile)[None, :]
    sums, pairs = [], []
    half = 1
    while half < tile:
        start = row // half * half
        later = row // half % 2 == 1
        sums.append(
            np.where(later, (col >= start) & (col <= row), (col > row) & (col < start + half))
        )
        pairs.append(later & (col // half == row // half - 1))
        half *= 2
    sums += [col <= row, col > row]
    pairs.append(row == col)
    return (
        np.concatenate(sums, 0).astype(np.float32),
        np.concatenate(pairs, 0).astype(np.float32),
        len(pairs) - 1,
    )


def dot(a, b, dims=None):
    if dims is None:
        return jnp.dot(a, b, preferred_element_type=F32)
    return lax.dot_general(a, b, dims, preferred_element_type=F32)


def layer_kernel(
    sizes,
    levels,
    cuts,
    finer,
    stream,
    gate_w,
    up_w,
    down_w,
    query_w,
    key_w,
    value_w,
    outgate_w,
    out_w,
    decay_down,
    decay_up,
    decay_bias,
    head_gain,
    norm_gain,
    span_sums,
    pair_masks,
    result,
    gate_all,
    up_all,
    down_all,
    qkvg_all,
    out_all,
    rows_all,
    part_out,
    part_in,
    cross_out,
    cross_in,
    partial,
    gate_buf,
    hidden,
    proj,
    log_gate,
    gated,
    state,
    guest_first,
    qkvg_w,
    proj_sums,
    decays,
    factors,
    w_send,
    w_recv,
    ag_send,
    ag_recv,
    fwd_send,
    rs_send,
    rs_recv,
    cross_send,
    cross_recv,
    guest_send,
    guest_recv,
    home_send,
    home_recv,
):
    reps, shards, ranks, cores = sizes
    chips = ranks // cores
    rep, shard, rank = lax.axis_index("rep"), lax.axis_index("fs"), lax.axis_index("tp")
    chip, core = rank // cores, lax.rem(rank, cores)
    block, width = stream.shape
    length = block * ranks
    half_rows = chips * block
    partner = {"tp": chip * cores + (cores - 1 - core)}

    barrier = pltpu.get_barrier_semaphore()

    def greet(device):
        pl.semaphore_signal(barrier, inc=1, device_id=device, device_id_type=MESH)

    @pl.when(shard > 0)
    def _():
        greet({"fs": shard - 1})

    @pl.when(shard < shards - 1)
    def _():
        greet({"fs": shard + 1})

    for step in range(1, reps):
        greet({"rep": lax.rem(rep + step, reps)})
    for step in range(1, ranks):
        greet({"tp": lax.rem(rank + step, ranks)})
    neighbours = (
        jnp.where(shard > 0, 1, 0) + jnp.where(shard < shards - 1, 1, 0) + reps - 1 + ranks - 1
    )
    lane = 0
    for w in (query_w, key_w, value_w, outgate_w):
        qkvg_w[:, lane : lane + w.shape[1]] = w[...]
        lane += w.shape[1]

    pl.semaphore_wait(barrier, neighbours)

    locals_ = (gate_w, up_w, down_w, qkvg_w, out_w)
    hosted = shards == HOSTED and cores > 1 and chips > 1
    guest = 3
    counts = (cuts, cuts, cuts, cuts * finer, cuts)
    starts = [sum(counts[:w]) for w in range(len(counts) + 1)]
    places = [(w, cut) for w in range(len(counts)) for cut in range(counts[w])]
    relayed = starts[3]
    items = starts[5]
    direct = range(cuts // 2, 3 * cuts)
    at_end = (shard == 0) | (shard == shards - 1)
    at_host = jnp.logical_not(at_end)
    near = jnp.where(shard < shards // 2, 0, shards - 1)
    home = jnp.where(shard < shards // 2, 1, shards - 2)
    far_host = shards - 1 - shard

    def is_host(at):
        return (at > 0) & (at < shards - 1)

    wholes = (gate_all, up_all, down_all, qkvg_all, out_all)

    def side_by_side(w):
        return wholes[w].shape[0] == locals_[w].shape[0]

    def piece(item, owner, part):
        w, cut = places[item]
        rows, columns = locals_[w].shape
        size = rows // (reps * counts[w])
        start = (part * counts[w] + cut) * size
        if side_by_side(w):
            return wholes[w].at[
                pl.ds(pl.multiple_of(start, size), size),
                pl.ds(pl.multiple_of(owner * columns, columns), columns),
            ]
        return wholes[w].at[pl.ds(pl.multiple_of(owner * rows + start, size), size), :]

    def own_piece(item, part=rep):
        w, cut = places[item]
        size = locals_[w].shape[0] // (reps * counts[w])
        start = pl.multiple_of((part * counts[w] + cut) * size, size)
        return locals_[w].at[pl.ds(start, size), :]

    def weight_copy(w, owner, part, slot, device, source=None):
        target = piece(w, owner, part)
        return pltpu.make_async_remote_copy(
            src_ref=target if source is None else source,
            dst_ref=target,
            send_sem=w_send.at[w, owner, slot],
            recv_sem=w_recv.at[w, owner, part],
            device_id=device,
            device_id_type=MESH,
        )

    def own_right(w):
        return weight_copy(w, shard, rep, 0, {"fs": shard + 1}, own_piece(w))

    def own_left(w):
        return weight_copy(w, shard, rep, reps, {"fs": shard - 1}, own_piece(w))

    def send_own(w):
        @pl.when(shard < shards - 1)
        def _():
            own_right(w).start()

        @pl.when(shard > 0)
        def _():
            own_left(w).start()

    def own_to(item, toward):
        slot = jnp.where(toward > shard, 0, reps)
        return weight_copy(item, shard, rep, slot, {"fs": toward}, own_piece(item))

    def own_rest(item):
        copies = []
        for step in range(1, reps):
            part = lax.rem(rep + step, reps)
            source = own_piece(item, part)
            copies.append(weight_copy(item, shard, part, step, {"fs": home}, source))
        return copies

    def keep_own(w):
        rows, columns = locals_[w].shape
        if side_by_side(w):
            at = pl.ds(pl.multiple_of(shard * columns, columns), columns)
            wholes[w][:, at] = locals_[w][...]
        else:
            wholes[w][pl.ds(pl.multiple_of(shard * rows, rows), rows), :] = locals_[w][...]

    def others(body, nearest=1, furthest=shards - 1):
        def at_distance(d, carry):
            for sign in (-1, 1):
                owner = shard + sign * d

                @pl.when((owner >= 0) & (owner < shards))
                def _():
                    body(owner, shard - sign)

            return carry

        lax.fori_loop(nearest, furthest + 1, at_distance, 0)

    def onto(item, owner, onward):
        return weight_copy(item, owner, rep, 0, {"fs": onward})

    def sideways(item, owner):
        return [
            weight_copy(item, owner, rep, step, {"rep": lax.rem(rep + step, reps)})
            for step in range(1, reps)
        ]

    def relay(item, nearest=1, furthest=shards - 1):
        def body(owner, onward):
            weight_copy(item, owner, rep, 0, partner).wait_recv()

            @pl.when((onward >= 0) & (onward < shards))
            def _():
                onto(item, owner, onward).start()

            for copy in sideways(item, owner):
                copy.start()

        others(body, nearest, furthest)

    def relay_from(item, owner, onward):
        weight_copy(item, owner, rep, 0, partner).wait_recv()
        onto(item, owner, onward).start()
        for copy in sideways(item, owner):
            copy.start()

    def pass_on(item):
        weight_copy(item, near, rep, 0, partner).wait_recv()
        onto(item, near, far_host).start()
        if item not in direct:
            for copy in sideways(item, near):
                copy.start()
        if item + HOST_AHEAD < relayed:
            own_to(item + HOST_AHEAD, far_host).start()

    def pass_across(item, owner):
        weight_copy(item, owner, rep, 0, partner).wait_recv()
        for copy in sideways(item, owner):
            copy.start()

    def send_late(item):
        def body(owner, onward):
            @pl.when(jnp.logical_not(is_host(onward)))
            def _():
                onto(item, owner, onward).start()

        others(body)

    def arrive(w):
        def body(owner, onward):
            for step in range(1, reps):
                weight_copy(w, owner, lax.rem(rep + step, reps), step, partner).wait_recv()

        others(body)

    def arrive_from(item, owner):
        for step in range(1, reps):
            weight_copy(item, owner, lax.rem(rep + step, reps), step, partner).wait_recv()

    def drain(item):
        @pl.when(shard < shards - 1)
        def _():
            own_right(item).wait_send()

        @pl.when(shard > 0)
        def _():
            own_left(item).wait_send()

        first = hosted and item in direct
        if first:

            @pl.when(at_end)
            def _():
                for copy in own_rest(item):
                    copy.wait_send()

        def body(owner, onward):
            @pl.when((onward >= 0) & (onward < shards))
            def _():
                onto(item, owner, onward).wait_send()

            @pl.when(jnp.logical_not(first & at_host & is_host(onward)))
            def _():
                for copy in sideways(item, owner):
                    copy.wait_send()

        others(body)

    def position(chip_at, core_at):
        return pl.multiple_of((core_at * chips + chip_at) * block, block)

    strip = block // PARTS

    fold = 2 if hosted else 1
    lap = block // fold

    def row_at(k, chip_at, core_at, offset):
        if k != 2:
            return position(chip_at, core_at) + offset
        return (chip_at * fold + offset // lap) * cores * lap + core_at * lap + offset % lap

    def row_copy(k, chip_at, core_at, send, part, device, source=None):
        at = pl.multiple_of(row_at(k, chip_at, core_at, part * strip), strip)
        target = rows_all.at[k, pl.ds(at, strip), :]
        return pltpu.make_async_remote_copy(
            src_ref=target if source is None else source.at[pl.ds(part * strip, strip), :],
            dst_ref=target,
            send_sem=send.at[part],
            recv_sem=ag_recv.at[k, core_at * chips + chip_at, part],
            device_id=device,
            device_id_type=MESH,
        )

    def guest_copy(part):
        at = pl.multiple_of(position(chip, core) + part * strip, strip)
        return pltpu.make_async_remote_copy(
            src_ref=stream.at[pl.ds(part * strip, strip), :],
            dst_ref=rows_all.at[guest, pl.ds(at, strip), :],
            send_sem=guest_send.at[part],
            recv_sem=guest_recv.at[part],
            device_id={"fs": home},
            device_id_type=MESH,
        )

    def home_copy(part):
        at = pl.multiple_of(position(chip, core) + part * strip, strip)
        return pltpu.make_async_remote_copy(
            src_ref=guest_first.at[pl.ds(part * strip, strip), :],
            dst_ref=rows_all.at[1, pl.ds(at, strip), :],
            send_sem=home_send.at[part],
            recv_sem=home_recv.at[part],
            device_id={"fs": near},
            device_id_type=MESH,
        )

    def chip_away(step):
        return lax.rem(chip + step, chips)

    def gather_own(k, part, source):
        copies = []
        for step in range(1, chips):
            device = {"tp": chip_away(step) * cores + core}
            copies.append(row_copy(k, chip, core, ag_send.at[k, step], part, device, source))
        if cores > 1:
            copies.append(row_copy(k, chip, core, ag_send.at[k, 0], part, partner, source))
        return copies

    def forward(k, step, part):
        return row_copy(k, chip_away(step), core, fwd_send.at[k, step], part, partner)

    def mirrored(k, step, part):
        return row_copy(
            k, chip_away(step), cores - 1 - core, fwd_send.at[k, step], part, partner
        )

    def gather_start(k, part, source):
        for copy in gather_own(k, part, source):
            copy.start()

    def gathered(k, body):
        gathered_near(k, body)
        gathered_away(k, body)

    def gathered_near(k, body):
        if cores > 1:
            for part in range(PARTS):
                mirrored(k, 0, part).wait_recv()

        def at_core(n, carry):
            body(pl.ds(pl.multiple_of(row_at(k, chip, n, 0), block), block))
            return carry

        lax.fori_loop(0, cores, at_core, 0)

    def gathered_away(k, body):
        for step in range(1, chips):
            for part in range(PARTS):
                forward(k, step, part).wait_recv()
                if cores > 1:
                    forward(k, step, part).start()

            def at_turn(n, carry):
                @pl.when(n == 1)
                def _():
                    for part in range(PARTS):
                        mirrored(k, step, part).wait_recv()

                turn = jnp.where(n == 0, core, cores - 1 - core)
                body(pl.ds(pl.multiple_of(row_at(k, chip_away(step), turn, 0), block), block))
                return carry

            lax.fori_loop(0, cores, at_turn, 0)

    def part_copy(k, chip_at):
        rows = pl.ds(pl.multiple_of(chip_at * block, block), block)
        return pltpu.make_async_remote_copy(
            src_ref=part_out.at[k, rows, :],
            dst_ref=part_in.at[k, rows, :],
            send_sem=rs_send.at[k, chip_at, 0],
            recv_sem=rs_recv.at[k, lax.rem(chip_at - chip + chips, chips), 0],
            device_id=partner,
            device_id_type=MESH,
        )

    def cross_copy(k, step, part):
        rows = pl.ds(part * strip, strip)
        return pltpu.make_async_remote_copy(
            src_ref=cross_out.at[k, step - 1, rows, :],
            dst_ref=cross_in.at[k, step - 1, rows, :],
            send_sem=cross_send.at[k, step - 1, part],
            recv_sem=cross_recv.at[k, step - 1, part],
            device_id={"tp": chip_away(step) * cores + core},
            device_id_type=MESH,
        )

    def product(k, left, weights, core_at, chip_at, into):
        depth, columns = weights.shape[0] // shards, weights.shape[1]
        at = row_at(k, chip_at, core_at, 0)
        rows = left[pl.ds(pl.multiple_of(at, block), block), :]
        to = pl.ds(pl.multiple_of(chip_at * block, block), block)

        def at_shard(j, carry):
            value = dot(rows, weights[pl.ds(pl.multiple_of(j * depth, depth), depth), :])
            into[to, pl.ds(pl.multiple_of(j * columns, columns), columns)] = value.astype(
                into.dtype
            )
            return carry

        lax.fori_loop(0, shards, at_shard, 0, unroll=hosted)

    def reduce_start(k, left, weights):
        sums = partial.at[k // 3]

        for step in range(1, chips + 1):
            away = chip_away(step)
            if cores > 1:
                product(k, left, weights, cores - 1 - core, away, part_out.at[k])
                part_copy(k, away).start()
            product(k, left, weights, core, away, sums)
            if step < chips:
                if cores > 1:
                    part_copy(k, away).wait_recv()
                for part in range(PARTS):
                    rows = pl.ds(pl.multiple_of(away * block + part * strip, strip), strip)
                    value = sums[rows, :]
                    if cores > 1:
                        value = value + part_in[k, rows, :].astype(F32)
                    cross_out[k, step - 1, part * strip : (part + 1) * strip, :] = value.astype(
                        BF16
                    )
                    cross_copy(k, step, part).start()
        if cores > 1:
            part_copy(k, chip).wait_recv()

    depth, columns = locals_[2].shape

    def block_at(chip_at, j):
        return (
            pl.ds(pl.multiple_of(chip_at * block, block), block),
            pl.ds(pl.multiple_of(j * columns, columns), columns),
        )

    def part_block(k, chip_at, j):
        at = block_at(chip_at, j)
        return pltpu.make_async_remote_copy(
            src_ref=part_out.at[k, at[0], at[1]],
            dst_ref=part_in.at[k, at[0], at[1]],
            send_sem=rs_send.at[k, chip_at, j],
            recv_sem=rs_recv.at[k, lax.rem(chip_at - chip + chips, chips), j],
            device_id=partner,
            device_id_type=MESH,
        )

    def cross_block(k, step, j):
        at = block_at(0, j)[1]
        return pltpu.make_async_remote_copy(
            src_ref=cross_out.at[k, step - 1, :, at],
            dst_ref=cross_in.at[k, step - 1, :, at],
            send_sem=cross_send.at[k, step - 1, j],
            recv_sem=cross_recv.at[k, step - 1, j],
            device_id={"tp": chip_away(step) * cores + core},
            device_id_type=MESH,
        )

    def block_product(k, core_at, chip_at, j):
        rows = pl.ds(pl.multiple_of(k // 3 * length + position(chip_at, core_at), block), block)
        return dot(hidden[rows, :], down_all[pl.ds(pl.multiple_of(j * depth, depth), depth), :])

    def block_parts(k, chip_at, j):
        rows, at = block_at(chip_at, j)
        part_out[k, rows, at] = block_product(k, cores - 1 - core, chip_at, j).astype(BF16)
        part_block(k, chip_at, j).start()
        partial[k // 3, rows, at] = block_product(k, core, chip_at, j)

    def block_cross(k, j):
        for step in range(1, chips):
            away = chip_away(step)
            rows, at = block_at(away, j)
            part_block(k, away, j).wait_recv()
            value = partial[k // 3, rows, at] + part_in[k, rows, at].astype(F32)
            cross_out[k, step - 1, :, at] = value.astype(BF16)
            cross_block(k, step, j).start()

    def reduce_blocks(owners, early=False):
        for k in (guest, 0):
            for j in owners:
                for step in range(1, chips):
                    block_parts(k, chip_away(step), j)
            if k == guest or early:
                for j in owners:
                    block_cross(k, j)

    def reduce_own(k):
        def at_shard(j, carry):
            block_parts(k, chip, j)
            return carry

        lax.fori_loop(0, shards, at_shard, 0)

    def blocks_landed(k):
        def at_shard(j, carry):
            part_block(k, chip, j).wait_recv()
            for step in range(1, chips):
                cross_block(k, step, j).wait_recv()
            return carry

        lax.fori_loop(0, shards, at_shard, 0)

    def drain_blocks(k):
        def at_shard(j, carry):
            for chip_at in range(chips):
                part_block(k, chip_at, j).wait_send()
            for step in range(1, chips):
                cross_block(k, step, j).wait_send()
            return carry

        lax.fori_loop(0, shards, at_shard, 0)

    def part_lap(chip_at, h):
        rows = pl.ds(pl.multiple_of(chip_at * block + h * lap, lap), lap)
        return pltpu.make_async_remote_copy(
            src_ref=part_out.at[2, rows, :],
            dst_ref=part_in.at[2, rows, :],
            send_sem=rs_send.at[2, chip_at, h],
            recv_sem=rs_recv.at[2, lax.rem(chip_at - chip + chips, chips), h],
            device_id=partner,
            device_id_type=MESH,
        )

    def lap_product(core_at, chip_at, h, into):
        left = pl.ds(pl.multiple_of(row_at(2, chip_at, core_at, h * lap), lap), lap)
        to = pl.ds(pl.multiple_of(chip_at * block + h * lap, lap), lap)

        def at_shard(j, carry):
            value = dot(hidden[left, :], down_all[pl.ds(pl.multiple_of(j * depth, depth), depth), :])
            into[to, pl.ds(pl.multiple_of(j * columns, columns), columns)] = value.astype(into.dtype)
            return carry

        lax.fori_loop(0, shards, at_shard, 0, unroll=True)

    def lap_parts(chip_at, h):
        lap_product(cores - 1 - core, chip_at, h, part_out.at[2])
        part_lap(chip_at, h).start()
        lap_product(core, chip_at, h, partial.at[0])

    def second_block():
        per_lap = PARTS // fold
        for part in range(PARTS):
            mirrored(2, 0, part).wait_recv()
        hidden_rows(pl.ds(pl.multiple_of(chip * cores * block, cores * block), cores * block))
        for h in range(fold):
            parts = range(h * per_lap, (h + 1) * per_lap)
            for step in range(1, chips):
                for part in parts:
                    forward(2, step, part).wait_recv()
                    forward(2, step, part).start()
            for step in range(1, chips):
                away = chip_away(step)
                for part in parts:
                    mirrored(2, step, part).wait_recv()
                at = (away * fold + h) * cores * lap
                hidden_rows(pl.ds(pl.multiple_of(at, cores * lap), cores * lap))
                if h == 0:
                    late_landed(2)
                lap_parts(away, h)
                part_lap(away, h).wait_recv()
                for part in parts:
                    rows = pl.ds(pl.multiple_of(away * block + part * strip, strip), strip)
                    value = partial[0, rows, :] + part_in[2, rows, :].astype(F32)
                    cross_out[2, step - 1, part * strip : (part + 1) * strip, :] = value.astype(BF16)
                    cross_copy(2, step, part).start()
        for h in range(fold):
            lap_parts(chip, h)
        for h in range(fold):
            part_lap(chip, h).wait_recv()

    def drain_laps():
        for h in range(fold):
            for chip_at in range(chips):
                part_lap(chip_at, h).wait_send()
        for part in range(PARTS):
            for step in range(1, chips):
                cross_copy(2, step, part).wait_send()

    chunk = min(32, strip)

    def finish_norm(k, part, scale, branch, into, into_at, blocks=False):
        if not blocks:
            for step in range(1, chips):
                cross_copy(k, step, part).wait_recv()

        def at_chunk(n, carry):
            rows = pl.ds(pl.multiple_of(chip * block + n * chunk, chunk), chunk)
            inner = pl.ds(pl.multiple_of(n * chunk, chunk), chunk)
            summed = partial[k // 3, rows, :]
            if cores > 1:
                summed = summed + part_in[k, rows, :].astype(F32)
            for step in range(1, chips):
                summed = summed + cross_in[k, step - 1, inner, :].astype(F32)
            current = rows_all[
                k, pl.ds(pl.multiple_of(row_at(k, chip, core, n * chunk), chunk), chunk), :
            ].astype(F32)
            values = RESIDUAL_SCALE * current + (summed if branch == 1.0 else branch * summed)
            centred = values - jnp.mean(values, -1, keepdims=True)
            spread = jnp.mean(centred * centred, -1, keepdims=True)
            done = (centred * lax.rsqrt(spread + NORM_EPS) * scale).astype(BF16)
            into[pl.ds(pl.multiple_of(into_at(n * chunk), chunk), chunk), :] = done
            return carry

        lax.fori_loop(part * strip // chunk, (part + 1) * strip // chunk, at_chunk, 0)

    def norm_to_rows(k, scale, branch, blocks=False, meanwhile=None):
        for part in range(PARTS):
            if meanwhile is not None:
                meanwhile(part)
            finish_norm(
                k, part, scale, branch, rows_all.at[k + 1],
                lambda offset: row_at(k + 1, chip, core, offset), blocks,
            )
            gather_start(k + 1, part, None)

    high = min(256, length)

    def by_rows(body):
        def at_rows(m, carry):
            body(pl.ds(pl.multiple_of(m * high, high), high))
            return carry

        lax.fori_loop(0, length // high, at_rows, 0)

    def silu(values):
        return values / (1.0 + jnp.exp(-values))

    def shifted(rows, slot):
        return pl.ds(pl.multiple_of(rows.start + slot * length, high), high)

    def gate_rows(rows, k=0, slot=0):
        gate_buf[shifted(rows, slot), :] = silu(dot(rows_all[k, rows, :], gate_all[...], NT))

    def up_rows(rows, k=0, slot=0):
        upward = dot(rows_all[k, rows, :], up_all[...], NT)
        at = shifted(rows, slot)
        hidden[at, :] = (gate_buf[at, :] * upward).astype(BF16)

    def both(rows_body):
        by_rows(rows_body)
        by_rows(lambda rows: rows_body(rows, guest, 1))

    def hidden_rows(rows):
        upward = dot(rows_all[2, rows, :], up_all[...], NT)
        gate = silu(dot(rows_all[2, rows, :], gate_all[...], NT))
        hidden[rows, :] = (gate * upward).astype(BF16)

    keys = decay_up.shape[1]
    heads = keys // DK
    vals = heads * DV

    furthest = jnp.where(at_end, shards - 1 - shard, shards - 1 - near)

    def slab(rows, j):
        deep = qkvg_w.shape[0]
        at = pl.ds(pl.multiple_of(j * deep, deep), deep)
        return dot(rows_all[1, rows, at], qkvg_all[at, :])

    def project_most(rows):
        decay_rows(rows)
        total = slab(rows, lax.rem(furthest + 1, shards))
        for step in range(2, shards):
            total = total + slab(rows, lax.rem(furthest + step, shards))
        proj_sums[rows, :] = total

    def project_last(rows):
        proj[rows, :] = (proj_sums[rows, :] + slab(rows, furthest)).astype(BF16)

    def project_rows(rows):
        decay_rows(rows)
        proj[rows, :] = dot(rows_all[1, rows, :], qkvg_all[...]).astype(BF16)

    def decay_rows(rows):
        low = dot(rows_all[1, rows, :], decay_down[...], NT).astype(BF16)
        pre = dot(low, decay_up[...]) + decay_bias[...]
        log_gate[rows, :] = (
            jnp.minimum(pre, 0.0) - jnp.log1p(jnp.exp(-jnp.abs(pre)))
        ) / GATE_DIVISOR

    bulk = keys % 128 == 0

    def spread(chip_at):
        span = cores * keys
        for n in range(cores):
            rows = pl.ds(position(chip_at, n), block)
            decay = log_gate[rows, :]
            coarse = decay.astype(BF16)
            lanes = slice(n * keys, (n + 1) * keys)
            decays[0:block, lanes] = coarse
            decays[block : 2 * block, lanes] = (decay - coarse.astype(F32)).astype(BF16)
        across = pl.ds(pl.multiple_of(chip_at * span, span), span)

        def at_table(at, carry):
            rows = pl.ds(pl.multiple_of(at * block, block), block)
            factors[rows, across] = jnp.exp(dot(span_sums[rows, :], decays[...]))
            return carry

        lax.fori_loop(0, levels + 2, at_table, 0, unroll=True)

    def mix():
        lane_head = lax.broadcasted_iota(jnp.int32, (1, keys), 1) // DK
        lane_masks = [jnp.where(lane_head == h, 1.0, 0.0) for h in range(heads)]
        state[...] = jnp.zeros_like(state)

        def at_tile(n, carry):
            rows = pl.ds(position(n // cores, lax.rem(n, cores)), block)
            query = proj[rows, 0:keys].astype(F32) * DK ** (-0.5)
            key_rows = proj[rows, keys : 2 * keys].astype(F32)
            value_rows = proj[rows, 2 * keys : 2 * keys + vals]
            decay = log_gate[rows, :]
            coarse = decay.astype(BF16)
            fine = (decay - coarse.astype(F32)).astype(BF16)

            def weight(at):
                if bulk:
                    lanes = pl.ds(pl.multiple_of(n * keys, keys), keys)
                    return factors[at * block : (at + 1) * block, lanes]
                table = span_sums[at * block : (at + 1) * block, 0:block]
                return jnp.exp(dot(table, coarse) + dot(table, fine))

            scores = [jnp.zeros((block, block), F32) for _ in range(heads)]
            for at in range(levels + 1):
                pairs = pair_masks[at * block : (at + 1) * block, :]
                if at < levels:
                    factor = weight(at)
                    late, early = query * factor, (key_rows * factor).astype(BF16)
                else:
                    late, early = query, key_rows.astype(BF16)
                for h in range(heads):
                    scores[h] = scores[h] + pairs * dot(
                        (late * lane_masks[h]).astype(BF16), early, NT
                    )
            ahead = weight(levels)
            behind = weight(levels + 1)
            late = query * ahead
            held = state[...].astype(BF16)
            for h in range(heads):
                lanes = slice(h * DV, (h + 1) * DV)
                mixed = dot(scores[h].astype(BF16), value_rows[:, lanes]) + dot(
                    (late * lane_masks[h]).astype(BF16), held[lanes, :], NT
                )
                outgate = proj[
                    rows, 2 * keys + vals + h * DV : 2 * keys + vals + (h + 1) * DV
                ].astype(F32)
                normed = (
                    mixed
                    * lax.rsqrt(jnp.mean(mixed * mixed, -1, keepdims=True) + HEAD_EPS)
                    * head_gain[...]
                )
                gated[rows, lanes] = (normed * (outgate / (1.0 + jnp.exp(-outgate)))).astype(BF16)
            state[...] = state[...] * ahead[block - 1 : block, :] + dot(
                value_rows, (key_rows * behind).astype(BF16), TN
            )
            return carry

        lax.fori_loop(0, ranks, at_tile, 0, unroll=True)

    def pull(start, stop):
        for item in range(start, stop):
            relay(item)
            if item + AHEAD < items:
                send_own(item + AHEAD)

    def landed(w):
        for item in range(starts[w], starts[w + 1]):
            arrive(item)

    own_at = pl.ds(position(chip, core), block)

    def opening():
        for item in range(min(AHEAD, items)):
            send_own(item)
        for part in range(PARTS):
            gather_start(0, part, stream)
        rows_all[0, own_at, :] = stream[...]
        for w in range(len(locals_)):
            keep_own(w)
        pull(0, cuts)
        gathered(0, lambda rows: None)
        pull(cuts, 2 * cuts)
        landed(0)
        by_rows(gate_rows)
        pull(2 * cuts, 3 * cuts)
        landed(1)
        by_rows(up_rows)
        pull(relayed, relayed + counts[3] // 2)
        landed(2)
        reduce_start(0, hidden, down_all)
        pull(relayed + counts[3] // 2, starts[4])
        norm_to_rows(0, norm_gain[0:1, :], BRANCH_SCALE)
        pull(starts[4], items)

    def opening_host():
        for item in range(min(HOST_AHEAD, relayed)):
            own_to(item, far_host).start()
        for part in range(PARTS):
            gather_start(0, part, stream)
        for item in range(relayed, items):
            own_to(item, near).start()
        for item in range(relayed):
            own_to(item, near).start()
        rows_all[0, own_at, :] = stream[...]
        for w in range(len(locals_)):
            keep_own(w)
        far_end = shards - 1 - near
        gates, ups, downs = (range(starts[w], starts[w + 1]) for w in range(3))
        for item in gates:
            pass_on(item)
            pass_across(item, far_host)
        for item in gates:
            pass_across(item, far_end)
        pass_across(cuts, far_host)
        for item in gates:
            send_late(item)
        for part in range(PARTS):
            guest_copy(part).wait_recv()
            gather_start(guest, part, None)
        for item in ups:
            pass_on(item)
        pass_across(cuts, far_end)
        gathered(0, lambda rows: None)
        for item in downs:
            pass_on(item)
        for item in ups[1:]:
            pass_across(item, far_host)
            pass_across(item, far_end)
        for item in range(relayed, items):
            own_to(item, far_host).start()
        for item in ups:
            onto(item, far_host, near).start()
        gathered(guest, lambda rows: None)
        landed(0)
        both(gate_rows)
        for item in downs:
            pass_across(item, far_host)
        pass_across(2 * cuts, far_end)
        landed(1)
        both(up_rows)
        for item in downs[1:]:
            pass_across(item, far_end)
        reduce_blocks([shard], True)
        down_items = range(2 * cuts, 3 * cuts)
        qkvg_items = range(relayed, starts[4])
        out_items = range(starts[4], items)
        for item in down_items:
            arrive_from(item, near)
        reduce_blocks([near], True)
        for item in (*qkvg_items, *out_items):
            relay_from(item, far_host, near)
        half = relayed + (starts[4] - relayed) // 2
        for item in range(relayed, half):
            relay_from(item, near, far_host)
        for item in down_items:
            arrive_from(item, far_host)
            arrive_from(item, far_end)
        reduce_blocks([far_host, far_end])
        for item in range(half, starts[4]):
            relay_from(item, near, far_host)
        for j in (far_host, far_end):
            block_cross(0, j)
        for item in range(relayed, half):
            relay_from(item, far_end, near)
        reduce_own(guest)
        reduce_own(0)
        blocks_landed(guest)
        for part in range(PARTS):
            finish_norm(guest, part, norm_gain[0:1, :], BRANCH_SCALE, guest_first, lambda offset: offset, True)
            home_copy(part).start()
        for item in range(half, starts[4]):
            relay_from(item, far_end, near)
        for item in out_items:
            relay_from(item, near, far_host)
        blocks_landed(0)
        norm_to_rows(0, norm_gain[0:1, :], BRANCH_SCALE, True)
        for item in out_items:
            relay_from(item, far_end, near)
        for item in ups:
            onto(item, far_end, near).start()
        for item in downs:
            send_late(item)

    def opening_end():
        for item in range(cuts):
            own_to(item, home).start()
        for part in range(PARTS):
            guest_copy(part).start()
        for item in range(cuts, relayed):
            own_to(item, home).start()
        for item in direct:
            for copy in own_rest(item):
                copy.start()
        for item in range(relayed, items):
            own_to(item, home).start()
        for w in range(len(locals_)):
            keep_own(w)
        for item in range(relayed, items):
            relay(item, 1, 1)
        for item in range(relayed):
            relay(item, 1, 1)
        for item in range(cuts):
            relay(item, 2)
        for item in range(cuts, 2 * cuts):
            relay(item, 2, 2)
        for item in range(relayed, starts[4]):
            relay(item, 2, 2)
        for item in range(starts[4], items):
            relay(item, 2, 2)
        half = relayed + (starts[4] - relayed) // 2
        for item in range(relayed, half):
            relay(item, 3)
        for part in range(PARTS):
            home_copy(part).wait_recv()
            gather_start(1, part, None)

    def late(start, stop, nearest=2):
        if hosted:

            @pl.when(at_end)
            def _():
                for item in range(start, stop):
                    relay(item, nearest)

    def late_landed(w):
        if hosted:

            @pl.when(at_end)
            def _():
                landed(w)

    def late_downs(part):
        if part == 1:
            late(2 * cuts, 2 * cuts + 1)
        if part == PARTS - 1:
            late(2 * cuts + 1, 3 * cuts)

    if hosted:
        pl.when(at_host)(opening_host)
        pl.when(at_end)(opening_end)
    else:
        opening()
    if hosted:
        for item in range(relayed, starts[4]):
            for step in range(1, shards):
                owner = lax.rem(furthest + step, shards)

                @pl.when(owner != shard)
                def _():
                    arrive_from(item, owner)

        gathered_near(1, project_most)
        half = relayed + (starts[4] - relayed) // 2
        late(half, starts[4] - 1, 3)
        if bulk:
            spread(chip)
        late(max(half, starts[4] - 1), starts[4], 3)
        gathered_away(1, project_most)
        late(starts[4], items, 3)
        if bulk:
            for step in range(1, chips):
                spread(chip_away(step))
        for item in range(relayed, starts[4]):
            arrive_from(item, furthest)
        by_rows(project_last)
    else:
        landed(3)
        gathered(1, project_rows)
        if bulk:
            for step in range(1, chips + 1):
                spread(chip_away(step))
    mix()
    late(cuts, cuts + 1, 3)
    landed(4)
    reduce_start(1, gated, out_all)
    late(cuts + 1, 2 * cuts, 3)
    norm_to_rows(
        1, norm_gain[1:2, :], 1.0, meanwhile=late_downs
    )
    late_landed(0)
    late_landed(1)
    if hosted:
        second_block()
    else:
        gathered(2, hidden_rows)
        reduce_start(2, hidden, down_all)
    for item in range(items):
        drain(item)

    def drain_rows(k, source=None):
        for part in range(PARTS):
            for copy in gather_own(k, part, source):
                copy.wait_send()
            for step in range(1, chips):
                if cores > 1:
                    forward(k, step, part).wait_send()

    def drain_sums(k):
        for part in range(PARTS):
            for step in range(1, chips):
                cross_copy(k, step, part).wait_send()
        if cores > 1:
            for chip_at in range(chips):
                part_copy(k, chip_at).wait_send()

    def drain_host():
        drain_rows(guest)
        drain_blocks(guest)
        for part in range(PARTS):
            home_copy(part).wait_send()

    def drain_end():
        for part in range(PARTS):
            guest_copy(part).wait_send()

    def drain_opening():
        drain_rows(0, stream)
        if hosted:
            drain_blocks(0)
        else:
            drain_sums(0)

    if hosted:

        @pl.when(at_host)
        def _():
            drain_opening()
            drain_host()

        pl.when(at_end)(drain_end)
    else:
        drain_opening()
    drain_rows(1)
    drain_sums(1)
    drain_rows(2)
    for part in range(PARTS):
        finish_norm(2, part, norm_gain[2:3, :], BRANCH_SCALE, result, lambda offset: offset)
    if hosted:
        drain_laps()
    else:
        drain_sums(2)


def solution(mesh):
    reps, shards, ranks = mesh.shape["rep"], mesh.shape["fs"], mesh.shape["tp"]
    cores = 2 if ranks % 2 == 0 else 1
    chips = ranks // cores

    def on_device(
        stream,
        gate_weight,
        up_weight,
        down_weight,
        query_weight,
        key_weight,
        value_weight,
        outgate_weight,
        decay_down,
        decay_up,
        decay_bias,
        head_gain,
        out_weight,
        norm_gain,
    ):
        projections = (query_weight, key_weight, value_weight, outgate_weight)
        qkvg = jax.ShapeDtypeStruct((query_weight.shape[0], sum(w.shape[1] for w in projections)), BF16)
        block, width = stream.shape
        length, half_rows = block * ranks, block * chips
        hidden_width = gate_weight.shape[1]
        keys = decay_up.shape[1]
        vals = value_weight.shape[1]
        sums, pairs, levels = level_tables(block)
        vmem = pl.BlockSpec(memory_space=pltpu.VMEM)
        away = max(chips - 1, 1)
        hosted = shards == HOSTED and cores > 1 and chips > 1
        phases, slots = (4, 2) if hosted else (3, 1)
        weights = (gate_weight.T, up_weight.T, down_weight, qkvg, out_weight)
        dma = pltpu.SemaphoreType.DMA
        cuts = max(c for c in (1, CUTS) if all(w.shape[0] % (16 * reps * c) == 0 for w in weights))
        finer = 2 if hosted and qkvg.shape[0] % (32 * reps * cuts) == 0 else 1
        pieces = cuts * (4 + finer)
        return pl.pallas_call(
            functools.partial(layer_kernel, (reps, shards, ranks, cores), levels, cuts, finer),
            out_shape=jax.ShapeDtypeStruct((block, width), BF16),
            in_specs=[vmem] * 16,
            out_specs=vmem,
            scratch_shapes=[
                *[pltpu.VMEM((w.shape[0], shards * w.shape[1]), BF16) for w in weights[:2]],
                *[pltpu.VMEM((shards * w.shape[0], w.shape[1]), BF16) for w in weights[2:]],
                pltpu.VMEM((phases, length, width), BF16),
                pltpu.VMEM((phases, half_rows, width), BF16),
                pltpu.VMEM((phases, half_rows, width), BF16),
                pltpu.VMEM((phases, away, block, width), BF16),
                pltpu.VMEM((phases, away, block, width), BF16),
                pltpu.VMEM((slots, half_rows, width), F32),
                pltpu.VMEM((slots * length, hidden_width), F32),
                pltpu.VMEM((slots * length, hidden_width), BF16),
                pltpu.VMEM((length, qkvg.shape[1]), BF16),
                pltpu.VMEM((length, keys), F32),
                pltpu.VMEM((length, vals), BF16),
                pltpu.VMEM((vals, keys), F32),
                pltpu.VMEM((block, width), BF16),
                pltpu.VMEM(qkvg.shape, BF16),
                pltpu.VMEM((length, qkvg.shape[1]), F32),
                pltpu.VMEM((2 * block, cores * keys), BF16),
                pltpu.VMEM(((levels + 2) * block, ranks * keys), F32),
                dma((pieces, shards, reps + 1)),
                dma((pieces, shards, reps)),
                dma((phases, chips, PARTS)),
                dma((phases, ranks, PARTS)),
                dma((phases, chips, PARTS)),
                dma((phases, chips, shards)),
                dma((phases, chips, shards)),
                dma((phases, away, max(PARTS, shards))),
                dma((phases, away, max(PARTS, shards))),
                *[dma((PARTS,))] * 4,
            ],
            compiler_params=pltpu.CompilerParams(
                collective_id=0, has_side_effects=True, vmem_limit_bytes=60 * 2**20
            ),
            name="layer",
        )(
            stream,
            *weights[:3],
            *projections,
            out_weight,
            decay_down.T,
            decay_up,
            decay_bias[None, :],
            head_gain[None, :],
            norm_gain,
            jnp.asarray(np.concatenate([sums, sums], 1), BF16),
            jnp.asarray(pairs, F32),
        )

    in_specs = (
        P(("rep", "fs", "tp"), None),
        P("fs", "tp"),
        P("fs", "tp"),
        P("tp", "fs"),
        P("fs", "tp"),
        P("fs", "tp"),
        P("fs", "tp"),
        P("fs", "tp"),
        P(),
        P(None, "tp"),
        P("tp"),
        P(),
        P("tp", "fs"),
        P(),
    )
    return jax.shard_map(
        on_device,
        mesh=mesh,
        in_specs=in_specs,
        out_specs=P(("rep", "fs", "tp"), None),
        check_vma=False,
    )
```
